32 devices in a mesh: rep: 2 (over x), fs: 8 (over z, y), tp: 2 (over core).
Axes of the slice: x: 2, y: 2, z: 4, core: 2. Of those that a mesh axis runs over, the one named last changes fastest.
Arguments:
- stream: bfloat16 [6144, 2048], P(('rep', 'fs'), 'tp'), may hold values from -24 to 24
- recurrence_input_weight: bfloat16 [2048, 2048], P('fs', 'tp'), may hold values from -0.125 to 0.125
- output_gate_weight: bfloat16 [2048, 2048], P('fs', 'tp'), may hold values from -0.125 to 0.125
- recurrence_gate_matrix: bfloat16 [16, 128, 128], P('tp'), may hold values from -0.5 to 0.5
- input_gate_matrix: bfloat16 [16, 128, 128], P('tp'), may hold values from -0.5 to 0.5
- channel_decay_rate: float32 [2048], P('tp')
- recurrence_taps: float32 [4, 2048], P(None, 'tp'), may hold values from -3 to 3
- spike_log_decay: float32 [6144, 16], P(('rep', 'fs'), 'tp'), may hold values from -2.1 to 0
- recurrence_output_weight: bfloat16 [2048, 2048], P('tp', 'fs'), may hold values from -0.3125 to 0.3125
- feedforward_gate_upward: bfloat16 [2048, 4096], P('fs', 'tp'), may hold values from -0.125 to 0.125
- feedforward_value_upward: bfloat16 [2048, 4096], P('fs', 'tp'), may hold values from -0.125 to 0.125
- feedforward_gate_taps: float32 [3, 4096], P(None, 'tp'), may hold values from -3 to 3
- feedforward_value_taps: float32 [3, 4096], P(None, 'tp'), may hold values from -3 to 3
- feedforward_down_weight: bfloat16 [4096, 2048], P('tp', 'fs'), may hold values from -0.1875 to 0.1875
- recurrence_norm_gain: float32 [2048], replicated, may hold values from 0.1 to 1.9
- feedforward_norm_gain: float32 [2048], replicated, may hold values from 0.1 to 1.9
- closing_norm_gain: float32 [2048], replicated, may hold values from 0.1 to 1.9
Outputs:
- layer_out: bfloat16 [6144, 2048], P(('rep', 'fs'), 'tp')
The draws below stay inside these ranges and needn't reach their ends.
All inputs are finite; a program needn't handle non-finite values.
Results may differ from the reference program's by a relative error of at most 0.018.
Values may be sent and summed in bfloat16 or wider, within the bound.
A program may use at most 64 MiB of HBM per device.

```python
import math
import jax
import jax.numpy as jnp
from jax import lax

MODEL_WIDTH = 2048
GATE_BLOCKS = 16
BLOCK = 128
R = 2048
FF = 4096
CONV = 4
FCONV = 3
SEQUENCE_TOKENS = 384
TOKEN_TOTAL = 6144
N_TP = 2


def draw_stream(key, part):
    row_key, sample_key = jax.random.split(jax.random.fold_in(key, 11), 2)
    samples = jax.random.truncated_normal(sample_key, -4.0, 4.0, (TOKEN_TOTAL, MODEL_WIDTH), jnp.float32)
    column_scale = jnp.exp(math.log(3.0) * jnp.arange(MODEL_WIDTH, dtype=jnp.float32) / MODEL_WIDTH)
    row_scale = jnp.exp(jax.random.uniform(row_key, (TOKEN_TOTAL, 1), jnp.float32, math.log(0.5), math.log(2.0)))
    return (samples * row_scale * column_scale[None, :]).astype(jnp.bfloat16)


def draw_channel_decay_rate(key, part):
    order_key, slow_key, fast_key = jax.random.split(jax.random.fold_in(key, 23), 3)
    ranking = jax.random.permutation(order_key, GATE_BLOCKS)
    slow_heads = ranking < GATE_BLOCKS // 2
    slow_rate = jnp.exp(jax.random.uniform(slow_key, (R,), jnp.float32, math.log(0.05), math.log(0.25))) / SEQUENCE_TOKENS
    fast_rate = jnp.exp(jax.random.uniform(fast_key, (R,), jnp.float32, math.log(0.006), math.log(0.025)))
    slow_mask = jnp.repeat(slow_heads, BLOCK)
    rate_per_step = jnp.where(slow_mask, slow_rate, fast_rate)
    return -jnp.log(jnp.expm1(rate_per_step))


def draw_spike_log_decay(key, part):
    position_random_key, depth_random_key = jax.random.split(jax.random.fold_in(key, 37), 2)
    sequence_count = TOKEN_TOTAL // SEQUENCE_TOKENS
    spike_positions = jax.random.randint(position_random_key, (sequence_count, 3, GATE_BLOCKS), 0, SEQUENCE_TOKENS)
    lower_limit = 0.5
    upper_limit = 0.8
    spike_depth = jnp.log(jax.random.uniform(depth_random_key, (sequence_count, 3, GATE_BLOCKS), jnp.float32, lower_limit, upper_limit))
    token_positions = jnp.arange(SEQUENCE_TOKENS)
    spike_hits = token_positions[None, None, :, None] == spike_positions[:, :, None, :]
    spike_total = jnp.sum(jnp.where(spike_hits, spike_depth[:, :, None, :], 0.0), axis=1)
    return spike_total.reshape(TOKEN_TOTAL, GATE_BLOCKS).astype(jnp.float32)


def steps_of(key, dims, shards, smallest, largest):
    factor_of = 1.0
    for dim, shards_of in shards:
        draws = jax.random.uniform(jax.random.fold_in(jax.random.fold_in(key, 6), dim), (shards_of,), jnp.float32, smallest / len(shards), largest / len(shards))
        factor_of = factor_of * jnp.repeat(jnp.exp(draws), dims[dim] // shards_of).reshape((-1,) + (1,) * (len(dims) - 1 - dim))
    return factor_of


def scatter_about(own_key, shape, spread, limit, shards=(), kind=jnp.bfloat16):
    result = jax.random.normal(own_key, shape, jnp.float32) * spread
    if len(shards) > 0:
        result = steps_of(own_key, shape, shards, -0.22, 0.18) * result
    return jnp.clip(result, min=-limit, max=limit).astype(kind)


def setup_inputs(seed: int = 0) -> dict:
    streams_of = jax.random.split(jax.random.key(seed), 18)
    stream = draw_stream(jax.random.fold_in(streams_of[17], 71), 0)
    recurrence_input_weight = scatter_about(streams_of[1], (MODEL_WIDTH, R), MODEL_WIDTH ** -0.5, 0.125, ((0, 8), (1, 2)))
    output_gate_weight = scatter_about(streams_of[2], (MODEL_WIDTH, R), MODEL_WIDTH ** -0.5, 0.125, ((0, 8), (1, 2)))
    recurrence_gate_matrix = scatter_about(streams_of[3], (GATE_BLOCKS, BLOCK, BLOCK), BLOCK ** -0.5, 0.5, ((0, 2),))
    input_gate_matrix = scatter_about(streams_of[4], (GATE_BLOCKS, BLOCK, BLOCK), BLOCK ** -0.5, 0.5, ((0, 2),))
    channel_decay_rate = draw_channel_decay_rate(jax.random.fold_in(streams_of[17], 71), 0)
    recurrence_taps = scatter_about(streams_of[6], (CONV, R), 0.5, 3.0, ((1, 2),), jnp.float32)
    spike_log_decay = draw_spike_log_decay(jax.random.fold_in(streams_of[17], 71), 0)
    recurrence_output_weight = scatter_about(streams_of[8], (R, MODEL_WIDTH), (R // 6) ** -0.5, 0.3125, ((0, 2), (1, 8)))
    feedforward_gate_upward = scatter_about(streams_of[9], (MODEL_WIDTH, FF), MODEL_WIDTH ** -0.5, 0.125, ((0, 8), (1, 2)))
    feedforward_value_upward = scatter_about(streams_of[10], (MODEL_WIDTH, FF), MODEL_WIDTH ** -0.5, 0.125, ((0, 8), (1, 2)))
    feedforward_gate_taps = scatter_about(streams_of[11], (FCONV, FF), 0.577, 3.0, ((1, 2),), jnp.float32)
    feedforward_value_taps = scatter_about(streams_of[12], (FCONV, FF), 0.577, 3.0, ((1, 2),), jnp.float32)
    feedforward_down_weight = scatter_about(streams_of[13], (FF, MODEL_WIDTH), (FF // 4) ** -0.5, 0.1875, ((0, 2), (1, 8)))
    recurrence_norm_gain = jnp.clip(1.0 + 0.18 * jax.random.normal(streams_of[14], (MODEL_WIDTH,), jnp.float32), 0.1, 1.9)
    feedforward_norm_gain = jnp.clip(1.0 + 0.18 * jax.random.normal(streams_of[15], (MODEL_WIDTH,), jnp.float32), 0.1, 1.9)
    closing_norm_gain = jnp.clip(1.0 + 0.18 * jax.random.normal(streams_of[16], (MODEL_WIDTH,), jnp.float32), 0.1, 1.9)
    return dict(stream=stream, recurrence_input_weight=recurrence_input_weight, output_gate_weight=output_gate_weight, recurrence_gate_matrix=recurrence_gate_matrix, input_gate_matrix=input_gate_matrix, channel_decay_rate=channel_decay_rate, recurrence_taps=recurrence_taps, spike_log_decay=spike_log_decay, recurrence_output_weight=recurrence_output_weight, feedforward_gate_upward=feedforward_gate_upward, feedforward_value_upward=feedforward_value_upward, feedforward_gate_taps=feedforward_gate_taps, feedforward_value_taps=feedforward_value_taps, feedforward_down_weight=feedforward_down_weight, recurrence_norm_gain=recurrence_norm_gain, feedforward_norm_gain=feedforward_norm_gain, closing_norm_gain=closing_norm_gain)


EPS = 1e-06
GATE_POWER = 8.0

def rms_scale(row_block, gain_vec):
    widened = row_block.astype(jnp.float32)
    inverse = lax.rsqrt(lax.optimization_barrier(jnp.mean(widened * widened, axis=-1, keepdims=True)) + EPS)
    return (widened * inverse * gain_vec).astype(jnp.bfloat16)

def causal_mix(values, kernel_taps):
    extent = kernel_taps.shape[0]
    length = values.shape[0]
    padded = jnp.pad(values, ((extent - 1, 0), (0, 0)))
    summed = kernel_taps[0] * padded[0:length]
    for offset in range(1, extent):
        summed = summed + kernel_taps[offset] * padded[offset:offset + length]
    return summed

def chain_step(earlier, following):
    return (earlier[0] * following[0], following[0] * earlier[1] + following[1])

def split_partials(left_rows, weight_rows, part_count):
    share_rows = left_rows.shape[1] // part_count
    summed = jnp.zeros((left_rows.shape[0], weight_rows.shape[1]), jnp.float32)
    for part_index in range(part_count):
        lower = part_index * share_rows
        partial_sum = jnp.dot(left_rows[:, lower:lower + share_rows], weight_rows[lower:lower + share_rows], preferred_element_type=jnp.float32).astype(jnp.bfloat16)
        summed = summed + lax.optimization_barrier(partial_sum).astype(jnp.float32)
    return summed

def reference(stream, recurrence_input_weight, output_gate_weight, recurrence_gate_matrix, input_gate_matrix, channel_decay_rate, recurrence_taps, spike_log_decay, recurrence_output_weight, feedforward_gate_upward, feedforward_value_upward, feedforward_gate_taps, feedforward_value_taps, feedforward_down_weight, recurrence_norm_gain, feedforward_norm_gain, closing_norm_gain):
    sequence_count = stream.shape[0] // SEQUENCE_TOKENS
    decay_base = (GATE_POWER * jax.nn.softplus(-channel_decay_rate)).reshape(GATE_BLOCKS, BLOCK)

    def single_sequence(input_rows):
        incoming_tokens, spike_events = input_rows
        normed = rms_scale(incoming_tokens, recurrence_norm_gain)
        rec_in = jnp.dot(normed, recurrence_input_weight, preferred_element_type=jnp.float32).astype(jnp.bfloat16)
        gate_src = jnp.dot(normed, output_gate_weight, preferred_element_type=jnp.float32).astype(jnp.bfloat16)
        conv_out = causal_mix(rec_in.astype(jnp.float32), recurrence_taps).astype(jnp.bfloat16)
        blocks = conv_out.astype(jnp.float32).reshape(SEQUENCE_TOKENS, GATE_BLOCKS, BLOCK)
        gate_restart = jax.nn.sigmoid(jnp.einsum('thi,hij->thj', blocks, recurrence_gate_matrix.astype(jnp.float32)))
        admit_gate = jax.nn.sigmoid(jnp.einsum('thi,hij->thj', blocks, input_gate_matrix.astype(jnp.float32)))
        decay_logarithm = -gate_restart * decay_base + spike_events[:, :, None]
        decay_rate = jnp.exp(decay_logarithm)
        inflow = jnp.sqrt(-jnp.expm1(2.0 * decay_logarithm)) * admit_gate * blocks
        states = lax.associative_scan(chain_step, (decay_rate, inflow), axis=0)[1]
        mixed_out = (states.reshape(SEQUENCE_TOKENS, R) * jax.nn.gelu(gate_src.astype(jnp.float32))).astype(jnp.bfloat16)
        branch = split_partials(mixed_out, recurrence_output_weight, N_TP).astype(jnp.bfloat16)
        middle = (incoming_tokens.astype(jnp.float32) + branch.astype(jnp.float32)).astype(jnp.bfloat16)
        normed_ffn = rms_scale(middle, feedforward_norm_gain)
        gate_up = jnp.dot(normed_ffn, feedforward_gate_upward, preferred_element_type=jnp.float32).astype(jnp.bfloat16)
        value_up = jnp.dot(normed_ffn, feedforward_value_upward, preferred_element_type=jnp.float32).astype(jnp.bfloat16)
        gate_conv = causal_mix(gate_up.astype(jnp.float32), feedforward_gate_taps)
        value_conv = causal_mix(value_up.astype(jnp.float32), feedforward_value_taps)
        hidden = (jax.nn.gelu(gate_conv) * value_conv).astype(jnp.bfloat16)
        branch_ffn = split_partials(hidden, feedforward_down_weight, N_TP).astype(jnp.bfloat16)
        final_rows = middle.astype(jnp.float32) + branch_ffn.astype(jnp.float32)
        inverse = lax.rsqrt(lax.optimization_barrier(jnp.mean(final_rows * final_rows, axis=-1, keepdims=True)) + EPS)
        return (final_rows * inverse * closing_norm_gain).astype(jnp.bfloat16)
    output_rows = lax.map(single_sequence, (stream.reshape(sequence_count, SEQUENCE_TOKENS, MODEL_WIDTH), spike_log_decay.reshape(sequence_count, SEQUENCE_TOKENS, GATE_BLOCKS)))
    return output_rows.reshape(sequence_count * SEQUENCE_TOKENS, MODEL_WIDTH)
```

```python
import functools

import jax
import jax.numpy as jnp
from jax import lax
from jax.experimental import pallas as pl
from jax.experimental.pallas import tpu as pltpu
from jax.sharding import PartitionSpec as P

EPS = 1e-06
GATE_POWER = 8.0


def rms_scale(row_block, gain_vec):
    widened = row_block.astype(jnp.float32)
    inverse = lax.rsqrt(jnp.mean(widened * widened, axis=-1, keepdims=True) + EPS)
    return (widened * inverse * gain_vec).astype(jnp.bfloat16)


def causal_mix(values, kernel_taps):
    extent = kernel_taps.shape[0]
    length = values.shape[0]
    padded = jnp.pad(values, ((extent - 1, 0), (0, 0)))
    summed = kernel_taps[0] * padded[0:length]
    for offset in range(1, extent):
        summed = summed + kernel_taps[offset] * padded[offset : offset + length]
    return summed


def chain_step(earlier, following):
    return (earlier[0] * following[0], following[0] * earlier[1] + following[1])


def fold_pair(source, pieces):
    return (
        jnp.dot(source, pieces[0], preferred_element_type=jnp.float32),
        jnp.dot(source, pieces[1], preferred_element_type=jnp.float32),
    )


def project_with(left_rows, weight_piece):
    return jnp.dot(left_rows, weight_piece, preferred_element_type=jnp.float32).astype(jnp.bfloat16)


class PairGather:
    def __init__(self, n, sources, targets, sems):
        self.n = n
        self.sources = sources
        self.targets = targets
        (self.local_sem, self.y_send, self.y_recv, self.z_send, self.z_recv, self.x_send, self.x_recv) = sems
        self.x = lax.axis_index("rep")
        fs = lax.axis_index("fs")
        self.y = lax.rem(fs, 2)
        self.z = fs // 2
        self.inner = jnp.logical_and(self.z > 0, self.z < n // 2 - 1)

    def level(self, k):
        if k == 0:
            return self.z
        if k == 1:
            return self.z + 1 - 2 * lax.rem(self.z, 2)
        if k == 2:
            return lax.rem(self.z + 2, 4)
        return 3 - self.z

    def side(self, q):
        return lax.rem(self.y + q, 2)

    def member(self, k, q):
        return 2 * self.level(k) + self.side(q)

    def enter(self):
        barrier = pltpu.get_barrier_semaphore()
        devices = [
            {"rep": 1 - self.x},
            {"tp": 1 - lax.axis_index("tp")},
            {"fs": self.member(0, 1)},
            {"fs": self.member(1, 0)},
            {"fs": self.member(2, 0)},
            {"fs": self.member(3, 0)},
        ]
        for device in devices:
            pl.semaphore_signal(
                barrier, inc=1, device_id=device, device_id_type=pl.DeviceIdType.MESH
            )
        pl.semaphore_wait(barrier, len(devices))

    def depth(self, w):
        return self.targets[w].shape[0] // self.n

    def source(self, w, half, r):
        ref, depth = self.sources[w], self.depth(w)
        part = depth // 2
        cols = self.targets[w].shape[1]
        if ref.shape[0] == depth:
            return ref.at[
                pl.ds(pl.multiple_of(r * part, 16), part),
                pl.ds(pl.multiple_of(half * cols, 128), cols),
            ]
        return ref.at[pl.ds(pl.multiple_of(half * depth + r * part, 16), part), :]

    def piece(self, w, shard, r):
        depth = self.depth(w)
        part = depth // 2
        return self.targets[w].at[pl.ds(pl.multiple_of(shard * depth + r * part, 16), part), :]

    def copy(self, source, target, send_sem, recv_sem, device):
        return pltpu.make_async_remote_copy(
            src_ref=source,
            dst_ref=target,
            send_sem=send_sem,
            recv_sem=recv_sem,
            device_id=device,
            device_id_type=pl.DeviceIdType.MESH,
        )

    def local(self, w, r):
        return pltpu.make_async_copy(
            self.source(w, self.y, r), self.piece(w, self.member(0, 0), r), self.local_sem.at[w, r]
        )

    def half_of(self, i):
        return self.x if i == 0 else 1 - self.x

    def y_copy(self, w, i):
        r = self.half_of(i)
        return self.copy(
            self.source(w, 1 - self.y, r),
            self.piece(w, self.member(0, 0), r),
            self.y_send.at[w, i],
            self.y_recv.at[w, i],
            {"fs": self.member(0, 1)},
        )

    def y_arrival(self, w, i):
        target = self.piece(w, self.member(0, 1), self.half_of(i))
        return self.copy(
            target, target, self.y_send.at[w, i], self.y_recv.at[w, i], {"fs": self.member(0, 1)}
        )

    def z_copy(self, w, q, k):
        target = self.piece(w, self.member(0, q), self.x)
        source = self.source(w, self.y, self.x) if q == 0 else target
        return self.copy(
            source,
            target,
            self.z_send.at[w, q, k],
            self.z_recv.at[w, q, k],
            {"fs": self.member(k, 0)},
        )

    def z_arrival(self, w, q, k):
        target = self.piece(w, self.member(k, q), self.x)
        return self.copy(
            target,
            target,
            self.z_send.at[w, q, k],
            self.z_recv.at[w, q, k],
            {"fs": self.member(k, 0)},
        )

    def z_forward(self, w, q):
        target = self.piece(w, self.member(2, q), self.x)
        return self.copy(
            target,
            target,
            self.z_send.at[w, q, 0],
            self.z_recv.at[w, q, 3],
            {"fs": self.member(1, 0)},
        )

    def x_copy(self, w, q, k):
        target = self.piece(w, self.member(k, q), self.x)
        return self.copy(
            target, target, self.x_send.at[w, q, k], self.x_recv.at[w, q, k], {"rep": 1 - self.x}
        )

    def x_arrival(self, w, q, k):
        target = self.piece(w, self.member(k, q), 1 - self.x)
        return self.copy(
            target, target, self.x_send.at[w, q, k], self.x_recv.at[w, q, k], {"rep": 1 - self.x}
        )

    def z_start(self, w, q):
        for k in (2, 1):
            self.z_copy(w, q, k).start()

        @pl.when(self.inner)
        def _():
            self.z_copy(w, q, 3).start()

    def cross(self, w):
        self.y_arrival(w, 0).wait_recv()
        self.z_start(w, 1)

    def serve(self, w, q, k):
        self.z_arrival(w, q, k).wait_recv()
        if k == 2:

            @pl.when(self.inner)
            def _():
                self.z_forward(w, q).start()

        self.x_copy(w, q, k).start()

    def own_ready(self, w):
        for r in (0, 1):
            self.local(w, r).wait()
        self.y_arrival(w, 1).wait_recv()

    def ready(self, w):
        self.own_ready(w)
        for q in (0, 1):
            for k in (1, 2, 3):
                self.x_arrival(w, q, k).wait_recv()

    def drain(self, w):
        for i in (0, 1):
            self.y_copy(w, i).wait_send()
        for q in (0, 1):
            for k in (1, 2):
                self.z_copy(w, q, k).wait_send()
            for k in (1, 2, 3):
                self.x_copy(w, q, k).wait_send()

            @pl.when(self.inner)
            def _():
                self.z_copy(w, q, 3).wait_send()
                self.z_forward(w, q).wait_send()


def gelu_of(x):
    return 0.5 * x * (1.0 + jnp.tanh(0.7978845608028654 * (x + 0.044715 * (x * x * x))))


def one_less_exp(z):
    series = 1.0 + z * (1.0 / 6.0)
    for order in (5.0, 4.0, 3.0, 2.0):
        series = 1.0 + z * (1.0 / order) * series
    return jnp.where(z > -0.35, -z * series, 1.0 - jnp.exp(z))


def tap_rows(values, taps_ref, cols):
    extent = taps_ref.shape[0]
    summed = taps_ref[extent - 1 : extent, cols] * values
    row = lax.broadcasted_iota(jnp.int32, values.shape, 0)
    for back in range(1, extent):
        moved = jnp.where(row >= back, pltpu.roll(values, back, 0), 0.0)
        summed = summed + taps_ref[extent - 1 - back : extent - back, cols] * moved
    return summed


def dot32(a, b):
    return jnp.dot(a, b, preferred_element_type=jnp.float32)


def layer_kernel(n, *refs):
    sources = refs[:6]
    (stream, reset_map, admit_map, decay_base, taps, spike) = refs[6:12]
    (gate_taps, value_taps, rec_gain, ffn_gain, last_gain, out) = refs[12:18]
    targets = refs[18:24]
    (whole, spike_in, normed, gate_src, decay, inflow, mixed) = refs[24:31]
    (away, landed, kept, share, share_in, middle, middle_in, gate_up, hidden) = refs[31:40]
    (terms, landed_down, down, down_own, down_in, final, sums, sums_in) = refs[40:48]
    gather_sems = refs[48:55]
    (keep_sem, pair_send, pair_recv, near_send, near_recv, far_send, far_recv) = refs[55:]
    tokens, width = stream.shape
    me = lax.axis_index("tp")
    gather = PairGather(n, sources, targets, gather_sems)
    side = gather.y
    bf16, f32 = jnp.bfloat16, jnp.float32
    tile = 256
    strip = 48
    channels = width // 2
    units = hidden.shape[1]
    chunks = 4
    chunk = 2 * tokens // chunks

    def near(i, source, target):
        return gather.copy(source, target, near_send.at[i], near_recv.at[i], {"tp": 1 - me})

    def far(i, source, target):
        return gather.copy(
            source, target, far_send.at[i], far_recv.at[i], {"fs": gather.member(0, 1)}
        )

    def pair(i, source, target):
        return gather.copy(source, target, pair_send.at[i], pair_recv.at[i], {"tp": 1 - me})

    def half(which):
        return pl.ds(pl.multiple_of(which * width, 128), width)

    def strips(lower, upper, body):
        def step(i, carry):
            body(pl.ds(pl.multiple_of(lower + i * strip, 16), strip))
            return carry

        lax.fori_loop(0, (upper - lower) // strip, step, 0)

    def norm_rows(lower, upper, mine, theirs, gain):
        def body(rows):
            a = mine(rows).astype(f32)
            b = theirs(rows).astype(f32)
            total = jnp.sum(a * a, axis=1, keepdims=True) + jnp.sum(b * b, axis=1, keepdims=True)
            inverse = lax.rsqrt(total * (1.0 / (2 * width)) + EPS)
            normed[rows, half(me)] = (a * inverse * gain[:, half(me)]).astype(bf16)
            normed[rows, half(1 - me)] = (b * inverse * gain[:, half(1 - me)]).astype(bf16)

        strips(lower, upper, body)

    first_rows, second_rows = pl.ds(0, tokens), pl.ds(tokens, tokens)
    mine_in = lambda rows: whole[rows, half(me)]
    theirs_in = lambda rows: whole[rows, half(1 - me)]

    arrivals = [(2, 0), (1, 0), (2, 1), (1, 1), (3, 0), (3, 1)]
    served = [0]

    def begin(w):
        gather.z_start(w, 0)
        gather.cross(w)

    def pump(upto):
        while served[0] < upto:
            at = served[0]
            w, step = at // 6, at % 6
            k, q = arrivals[step]
            gather.serve(w, q, k)
            served[0] = at + 1
            if step == 3 and w + 2 < 6:
                begin(w + 2)
            if at == 6:
                for i in (0, 1):
                    for later in (3, 4, 5):
                        gather.y_copy(later, i).start()

    gather.enter()
    own_half = near(0, stream, whole.at[first_rows, half(me)])
    own_half.start()
    for w in range(3):
        gather.y_copy(w, 0).start()
    gather.z_start(0, 0)
    sent_half = far(0, stream, whole.at[second_rows, half(me)])
    sent_half.start()
    sent_spike = far(1, spike, spike_in)
    sent_spike.start()
    for w in range(3):
        gather.y_copy(w, 1).start()
    keep = pltpu.make_async_copy(stream, whole.at[first_rows, half(me)], keep_sem.at[0])
    keep.start()
    for w in range(6):
        for r in (0, 1):
            gather.local(w, r).start()
    gather.cross(0)
    begin(1)
    pump(4)
    keep.wait()
    own_half.wait()
    norm_rows(0, tokens, mine_in, theirs_in, rec_gain)
    pump(6)
    sent_half.wait()
    sent_spike.wait()
    passed = whole.at[second_rows, half(me)]
    pass_on = near(1, passed, passed)
    pass_on.start()
    pump(8)
    pass_on.wait()
    norm_rows(tokens, 2 * tokens, mine_in, theirs_in, rec_gain)
    pump(14)
    gather.ready(0)
    gather.ready(1)

    row_sets = [pl.ds(s * tokens, tokens) for s in (0, 1)]
    base = side * channels

    def wide(start, size):
        return pl.ds(pl.multiple_of(start, 128), size)

    for c in range(channels // tile):
        cols = slice(c * tile, (c + 1) * tile)
        for s in (0, 1):
            rows = row_sets[s]
            rec = dot32(normed[rows, :], targets[0][:, cols]).astype(bf16).astype(f32)
            conv = tap_rows(rec, taps, wide(base + c * tile, tile)).astype(bf16)
            gate_src[rows, cols] = dot32(normed[rows, :], targets[1][:, cols]).astype(bf16)
            spikes = spike if s == 0 else spike_in
            for part in range(tile // 128):
                h = c * (tile // 128) + part
                heads = channels // 128
                lanes = slice(h * 128, (h + 1) * 128)
                block = conv[:, part * 128 : (part + 1) * 128]
                reset = jax.nn.sigmoid(dot32(block, reset_map[side * heads + h]))
                admit = jax.nn.sigmoid(dot32(block, admit_map[side * heads + h]))
                events = jnp.where(
                    side == 0, spikes[:, h : h + 1], spikes[:, heads + h : heads + h + 1]
                )
                log_decay = events - reset * decay_base[:, wide(base + h * 128, 128)]
                decay[rows, lanes] = jnp.exp(log_decay)
                inflow[rows, lanes] = (
                    jnp.sqrt(one_less_exp(2.0 * log_decay)) * admit * block.astype(f32)
                )
            pump(15 + 2 * c + s)

    row = lax.broadcasted_iota(jnp.int32, (8, channels), 0)

    def scan_step(i, carry):
        passed_on = []
        for s in (0, 1):
            rows = pl.ds(pl.multiple_of(s * tokens + i * 16, 16), 16)
            a16, b16 = decay[rows, :], inflow[rows, :]
            state = carry[s]
            found = []
            for part in range(2):
                a, b = a16[part * 8 : part * 8 + 8], b16[part * 8 : part * 8 + 8]
                for back in (1, 2, 4):
                    a_before = jnp.where(row >= back, pltpu.roll(a, back, 0), 1.0)
                    b_before = jnp.where(row >= back, pltpu.roll(b, back, 0), 0.0)
                    b = a * b_before + b
                    a = a * a_before
                states = a * state + b
                state = states[7:8, :]
                found.append(states)
            states = jnp.concatenate(found, axis=0)
            mixed[rows, :] = (states * gelu_of(gate_src[rows, :].astype(f32))).astype(bf16)
            passed_on.append(state)
        return tuple(passed_on)

    still = jnp.zeros((1, channels), f32)
    halfway = tokens // 32
    carry = lax.fori_loop(0, halfway, scan_step, (still, still))
    pump(19)
    lax.fori_loop(halfway, tokens // 16, scan_step, carry)
    gather.ready(2)

    per_half = n // 2
    depth = channels

    def block_of(w, slot, depth):
        return targets[w][pl.ds(pl.multiple_of(slot * depth, 16), depth), :]

    def away_step(j, carry):
        cols = wide(j * tile, tile)
        away[:, cols] = dot32(mixed[...], block_of(2, (1 - me) * per_half + j, depth)).astype(bf16)
        near(2 + j, away.at[:, cols], landed.at[:, cols]).start()
        return carry

    def keep_step(j, carry):
        cols = wide(j * tile, tile)
        kept[:, cols] = dot32(mixed[...], block_of(2, me * per_half + j, depth)).astype(bf16)
        return carry

    lax.fori_loop(0, per_half, away_step, 0)
    lax.fori_loop(0, per_half, keep_step, 0)
    for j in range(per_half):
        cols = slice(j * tile, (j + 1) * tile)
        near(2 + j, away.at[:, cols], landed.at[:, cols]).wait()

    def share_rows(rows):
        share[rows, :] = (kept[rows, :].astype(f32) + landed[rows, :].astype(f32)).astype(bf16)

    def share_copy(i):
        rows = pl.ds((i + chunks // 2) % chunks * chunk, chunk)
        return far(2 + i, share.at[rows, :], share_in.at[pl.ds(i * chunk, chunk), :])

    def middle_copy(i):
        rows = pl.ds(i * chunk, chunk)
        return pair(i, middle.at[rows, :], middle_in.at[rows, :])

    for i in range(chunks):
        lower = (i + chunks // 2) % chunks * chunk
        strips(lower, lower + chunk, share_rows)
        share_copy(i).start()

    def add_branch(rows):
        branch = (share[rows, :].astype(f32) + share_in[rows, :].astype(f32)).astype(bf16)
        middle[rows, :] = (whole[rows, half(me)].astype(f32) + branch.astype(f32)).astype(bf16)

    for i in range(chunks):
        pump((20, 22, 23, 24)[i])
        share_copy(i).wait()
        strips(i * chunk, (i + 1) * chunk, add_branch)
        middle_copy(i).start()
        pump((21, 22, 23, 25)[i])
        middle_copy(i).wait()
        norm_rows(
            i * chunk,
            (i + 1) * chunk,
            lambda rows: middle[rows, :],
            lambda rows: middle_in[rows, :],
            ffn_gain,
        )
    gather.ready(3)

    unit_base = side * units
    tiles = units // tile

    def gate_step(j, carry):
        cols = wide(j * tile, tile)
        gate_up[:, cols] = dot32(normed[...], targets[3][:, cols]).astype(bf16)
        return carry

    for j in range(tiles):
        lax.fori_loop(j, j + 1, gate_step, 0)
        pump(26 + j // 2)
    pump(31)
    gather.ready(4)

    def up_step(j, carry):
        cols = wide(j * tile, tile)
        for s in (0, 1):
            rows = row_sets[s]
            picked = wide(unit_base + j * tile, tile)
            value = dot32(normed[rows, :], targets[4][:, cols]).astype(bf16).astype(f32)
            value = tap_rows(value, value_taps, picked)
            gate = gelu_of(tap_rows(gate_up[rows, cols].astype(f32), gate_taps, picked))
            hidden[rows, cols] = (gate * value).astype(bf16)
        return carry

    for j in range(tiles):
        lax.fori_loop(j, j + 1, up_step, 0)
        pump(min(32 + j, 34))

    low = gather.z // 2
    order = [(0, 0), (0, 1)] + arrivals

    def owned(k):
        return (me == low) if k in (0, 1) else (me == 1 - low)

    def slot_of(i):
        k, q = order[i]
        return gather.member(k, q)

    def down_copy(i):
        cols = wide(slot_of(i) * tile, tile)
        place = wide(lax.rem(slot_of(i), per_half) * tile, tile)
        return near(2 + per_half + i, terms.at[:, cols], landed_down.at[:, place])

    def down_far(i):
        place = wide(lax.rem(slot_of(i), per_half) * tile, tile)
        slot = lax.rem(slot_of(i), per_half)
        return gather.copy(
            down.at[:, place],
            down_in.at[:, place],
            far_send.at[2 + chunks + slot],
            far_recv.at[2 + chunks + slot],
            {"fs": gather.member(0, 1)},
        )

    def fold(i):
        @pl.when(owned(order[i][0]))
        def _():
            down_copy(i).wait_recv()
            cols = wide(slot_of(i) * tile, tile)
            place = wide(lax.rem(slot_of(i), per_half) * tile, tile)

            def far_rows(r, carry):
                rows = pl.ds(pl.multiple_of(r * 128, 16), 128)
                later = pl.ds(pl.multiple_of(tokens + r * 128, 16), 128)
                down[rows, place] = (
                    terms[later, cols].astype(f32) + landed_down[later, place].astype(f32)
                ).astype(bf16)
                return carry

            lax.fori_loop(0, tokens // 128, far_rows, 0)
            down_far(i).start()

            def own_rows(r, carry):
                rows = pl.ds(pl.multiple_of(r * 128, 16), 128)
                down_own[rows, place] = (
                    terms[rows, cols].astype(f32) + landed_down[rows, place].astype(f32)
                ).astype(bf16)
                return carry

            lax.fori_loop(0, tokens // 128, own_rows, 0)

    for i in range(len(order)):
        k, q = order[i]
        if k == 0 and q == 0:
            gather.own_ready(5)
        if k > 0:
            pump(min(30 + i, 36))
            gather.x_arrival(5, q, k).wait_recv()
        cols = wide(slot_of(i) * tile, tile)
        terms[:, cols] = dot32(hidden[...], block_of(5, slot_of(i), units)).astype(bf16)

        @pl.when(jnp.logical_not(owned(k)))
        def _():
            down_copy(i).start()

        if i > 0:
            fold(i - 1)
    fold(len(order) - 1)
    for i in range(len(order)):

        @pl.when(owned(order[i][0]))
        def _():
            down_far(i).wait()

        @pl.when(jnp.logical_not(owned(order[i][0])))
        def _():
            down_copy(i).wait_send()

    def finish(rows):
        branch = (down_own[rows, :].astype(f32) + down_in[rows, :].astype(f32)).astype(bf16)
        total = middle[rows, :].astype(f32) + branch.astype(f32)
        final[rows, :] = total
        square = jnp.sum(total * total, axis=1, keepdims=True)
        sums[rows, :] = jnp.broadcast_to(square, (strip, 128))

    strips(0, tokens, finish)
    summed = pair(chunks, sums, sums_in)
    summed.start()
    summed.wait()

    def scale(rows):
        square = sums[rows, :] + sums_in[rows, :]
        inverse = lax.rsqrt(square * (1.0 / (2 * width)) + EPS)[:, 0:1]
        out[rows, :] = (final[rows, :] * inverse * last_gain[:, half(me)]).astype(bf16)

    strips(0, tokens, scale)
    for w in range(6):
        gather.drain(w)


def fused_layer(n, weights, others):
    tokens, width = others[0].shape
    units = weights[3].shape[1] // 2
    channels = width // 2
    bf16, f32 = jnp.bfloat16, jnp.float32
    vmem = pltpu.VMEM
    dma = pltpu.SemaphoreType.DMA
    halves = []
    for w in weights:
        if w.shape[0] == 2 * width // n:
            halves.append((n * w.shape[0], w.shape[1] // 2))
        else:
            halves.append((n * w.shape[0] // 2, w.shape[1]))
    both = 2 * tokens
    return pl.pallas_call(
        functools.partial(layer_kernel, n),
        out_shape=jax.ShapeDtypeStruct((tokens, width), bf16),
        in_specs=[pl.BlockSpec(memory_space=pl.ANY)] * 6
        + [pl.BlockSpec(memory_space=vmem)] * len(others),
        out_specs=pl.BlockSpec(memory_space=vmem),
        scratch_shapes=[vmem(shape, w.dtype) for shape, w in zip(halves, weights)]
        + [
            vmem((both, 2 * width), bf16),
            vmem(others[5].shape, f32),
            vmem((both, 2 * width), bf16),
            vmem((both, channels), bf16),
            vmem((both, channels), f32),
            vmem((both, channels), f32),
            vmem((both, channels), bf16),
            vmem((both, width), bf16),
            vmem((both, width), bf16),
            vmem((both, width), bf16),
            vmem((both, width), bf16),
            vmem((both, width), bf16),
            vmem((both, width), bf16),
            vmem((both, width), bf16),
            vmem((both, units), bf16),
            vmem((both, units), bf16),
            vmem((both, 2 * width), bf16),
            vmem((both, width), bf16),
            vmem((tokens, width), bf16),
            vmem((tokens, width), bf16),
            vmem((tokens, width), bf16),
            vmem((tokens, width), f32),
            vmem((tokens, 128), f32),
            vmem((tokens, 128), f32),
            dma((6, 2)),
            dma((6, 2)),
            dma((6, 2)),
            dma((6, 2, 4)),
            dma((6, 2, 4)),
            dma((6, 2, 4)),
            dma((6, 2, 4)),
            dma((1,)),
            dma((5,)),
            dma((5,)),
            dma((2 + n // 2 + n,)),
            dma((2 + n // 2 + n,)),
            dma((6 + n // 2,)),
            dma((6 + n // 2,)),
        ],
        compiler_params=pltpu.CompilerParams(
            collective_id=0, has_side_effects=True, vmem_limit_bytes=66_000_000
        ),
    )(*weights, *others)


def shards(
    ringed,
    stream,
    recurrence_input_weight,
    output_gate_weight,
    recurrence_gate_matrix,
    input_gate_matrix,
    channel_decay_rate,
    recurrence_taps,
    spike_log_decay,
    recurrence_output_weight,
    feedforward_gate_upward,
    feedforward_value_upward,
    feedforward_gate_taps,
    feedforward_value_taps,
    feedforward_down_weight,
    recurrence_norm_gain,
    feedforward_norm_gain,
    closing_norm_gain,
):
    tok_rows = stream.shape[0]
    fs_size = lax.axis_size("fs")
    if ringed:
        return fused_layer(
            fs_size,
            (
                recurrence_input_weight,
                output_gate_weight,
                recurrence_output_weight,
                feedforward_gate_upward,
                feedforward_value_upward,
                feedforward_down_weight,
            ),
            (
                stream,
                recurrence_gate_matrix,
                input_gate_matrix,
                (GATE_POWER * jax.nn.softplus(-channel_decay_rate))[None, :],
                recurrence_taps,
                spike_log_decay,
                feedforward_gate_taps,
                feedforward_value_taps,
                recurrence_norm_gain[None, :],
                feedforward_norm_gain[None, :],
                closing_norm_gain[None, :],
            ),
        )
    weights = [
        lax.all_gather(recurrence_input_weight, "fs", axis=0, tiled=True),
        lax.all_gather(output_gate_weight, "fs", axis=0, tiled=True),
        lax.all_gather(recurrence_output_weight, "fs", axis=1, tiled=True),
        lax.all_gather(feedforward_gate_upward, "fs", axis=0, tiled=True),
        lax.all_gather(feedforward_value_upward, "fs", axis=0, tiled=True),
        lax.all_gather(feedforward_down_weight, "fs", axis=1, tiled=True),
    ]
    head_count = recurrence_gate_matrix.shape[0]
    block_size = recurrence_gate_matrix.shape[1]
    whole_rows = lax.all_gather(stream, "tp", axis=1, tiled=True)
    normed = rms_scale(whole_rows, recurrence_norm_gain)
    rec_sum, gate_sum = fold_pair(
        normed,
        (
            weights[0],
            weights[1],
        ),
    )
    rec_in = rec_sum.astype(jnp.bfloat16)
    gate_src = gate_sum.astype(jnp.bfloat16)
    conv_out = causal_mix(rec_in.astype(jnp.float32), recurrence_taps).astype(jnp.bfloat16)
    blocks = conv_out.reshape(tok_rows, head_count, block_size)
    gate_restart = jax.nn.sigmoid(
        jnp.einsum(
            "thi,hij->thj", blocks, recurrence_gate_matrix, preferred_element_type=jnp.float32
        )
    )
    admit_gate = jax.nn.sigmoid(
        jnp.einsum("thi,hij->thj", blocks, input_gate_matrix, preferred_element_type=jnp.float32)
    )
    decay_base = (GATE_POWER * jax.nn.softplus(-channel_decay_rate)).reshape(head_count, block_size)
    decay_logarithm = -gate_restart * decay_base + spike_log_decay[:, :, None]
    decay_rate = jnp.exp(decay_logarithm)
    inflow = jnp.sqrt(-jnp.expm1(2.0 * decay_logarithm)) * admit_gate * blocks.astype(jnp.float32)
    states = lax.associative_scan(chain_step, (decay_rate, inflow), axis=0)[1]
    mixed_out = (
        states.reshape(tok_rows, head_count * block_size)
        * jax.nn.gelu(gate_src.astype(jnp.float32))
    ).astype(jnp.bfloat16)
    mix_terms = project_with(
        mixed_out, weights[2]
    )
    branch = lax.psum_scatter(
        lax.optimization_barrier(mix_terms).astype(jnp.float32).astype(jnp.bfloat16),
        "tp",
        scatter_dimension=1,
        tiled=True,
    )
    middle = (stream.astype(jnp.float32) + branch.astype(jnp.float32)).astype(jnp.bfloat16)
    whole_middle = lax.all_gather(middle, "tp", axis=1, tiled=True)
    normed_ffn = rms_scale(whole_middle, feedforward_norm_gain)
    gate_sum_ffn, value_sum_ffn = fold_pair(
        normed_ffn,
        (
            weights[3],
            weights[4],
        ),
    )
    gate_up = gate_sum_ffn.astype(jnp.bfloat16)
    value_up = value_sum_ffn.astype(jnp.bfloat16)
    gate_conv = causal_mix(gate_up.astype(jnp.float32), feedforward_gate_taps)
    value_conv = causal_mix(value_up.astype(jnp.float32), feedforward_value_taps)
    hidden = (jax.nn.gelu(gate_conv) * value_conv).astype(jnp.bfloat16)
    down_terms = project_with(
        hidden, weights[5]
    )
    branch_ffn = lax.psum_scatter(
        lax.optimization_barrier(down_terms).astype(jnp.float32).astype(jnp.bfloat16),
        "tp",
        scatter_dimension=1,
        tiled=True,
    )
    final_rows = middle.astype(jnp.float32) + branch_ffn.astype(jnp.float32)
    col_count = final_rows.shape[1]
    square_sum = lax.psum(jnp.sum(final_rows * final_rows, axis=1), "tp")
    inverse = lax.rsqrt(square_sum / (col_count * lax.axis_size("tp")) + EPS)
    gain_part = lax.dynamic_slice_in_dim(
        closing_norm_gain, lax.axis_index("tp") * col_count, col_count
    )
    return (final_rows * inverse[:, None] * gain_part[None, :]).astype(jnp.bfloat16)


def solution(mesh):
    in_specs = (
        P(("rep", "fs"), "tp"),
        P("fs", "tp"),
        P("fs", "tp"),
        P("tp", None, None),
        P("tp", None, None),
        P("tp"),
        P(None, "tp"),
        P(("rep", "fs"), "tp"),
        P("tp", "fs"),
        P("fs", "tp"),
        P("fs", "tp"),
        P(None, "tp"),
        P(None, "tp"),
        P("tp", "fs"),
        P(),
        P(),
        P(),
    )
    out_specs = P(("rep", "fs"), "tp")
    ringed = mesh.shape["rep"] == 2 and mesh.shape["tp"] == 2 and mesh.shape["fs"] == 8
    body = functools.partial(shards, ringed)
    return jax.shard_map(body, mesh=mesh, in_specs=in_specs, out_specs=out_specs, check_vma=False)
```

```python
import functools

import jax
import jax.numpy as jnp
from jax import lax
from jax.experimental import pallas as pl
from jax.experimental.pallas import tpu as pltpu
from jax.sharding import PartitionSpec as P

EPS = 1e-06
GATE_POWER = 8.0


def rms_scale(row_block, gain_vec):
    widened = row_block.astype(jnp.float32)
    inverse = lax.rsqrt(jnp.mean(widened * widened, axis=-1, keepdims=True) + EPS)
    return (widened * inverse * gain_vec).astype(jnp.bfloat16)


def causal_mix(values, kernel_taps):
    extent = kernel_taps.shape[0]
    length = values.shape[0]
    padded = jnp.pad(values, ((extent - 1, 0), (0, 0)))
    summed = kernel_taps[0] * padded[0:length]
    for offset in range(1, extent):
        summed = summed + kernel_taps[offset] * padded[offset : offset + length]
    return summed


def chain_step(earlier, following):
    return (earlier[0] * following[0], following[0] * earlier[1] + following[1])


def fold_pair(source, pieces):
    return (
        jnp.dot(source, pieces[0], preferred_element_type=jnp.float32),
        jnp.dot(source, pieces[1], preferred_element_type=jnp.float32),
    )


def project_with(left_rows, weight_piece):
    return jnp.dot(left_rows, weight_piece, preferred_element_type=jnp.float32).astype(jnp.bfloat16)


class PairGather:
    def __init__(self, n, sources, targets, shifts, sems):
        self.n = n
        self.shifts = shifts
        self.sources = sources
        self.targets = targets
        (self.local_sem, self.y_send, self.y_recv, self.z_send, self.z_recv, self.x_send, self.x_recv) = sems
        self.x = lax.axis_index("rep")
        fs = lax.axis_index("fs")
        self.y = lax.rem(fs, 2)
        self.z = fs // 2
        levels = n // 2
        self.middle = self.z * (levels - 1 - self.z) // (levels - 2)
        self.inner = self.middle == 1

    def level(self, k):
        levels = self.n // 2
        across = levels - 1 - self.z
        beyond = lax.rem(self.z + levels // 2, levels)
        if k == 0:
            return self.z
        if k == 1:
            return self.z + 1 - 2 * lax.rem(self.z, 2)
        if k == 2:
            return self.middle * across + (1 - self.middle) * beyond
        return self.middle * beyond + (1 - self.middle) * across

    def side(self, q):
        return lax.rem(self.y + q, 2)

    def member(self, k, q):
        return 2 * self.level(k) + self.side(q)

    def enter(self):
        barrier = pltpu.get_barrier_semaphore()
        devices = [
            {"rep": 1 - self.x},
            {"tp": 1 - lax.axis_index("tp")},
            {"fs": self.member(0, 1)},
            {"fs": self.member(1, 0)},
        ]
        for device in devices:
            pl.semaphore_signal(
                barrier, inc=1, device_id=device, device_id_type=pl.DeviceIdType.MESH
            )

        @pl.when(self.inner)
        def _():
            pl.semaphore_signal(
                barrier,
                inc=1,
                device_id={"fs": self.member(2, 0)},
                device_id_type=pl.DeviceIdType.MESH,
            )

        pl.semaphore_wait(barrier, len(devices) + self.middle)

    def depth(self, w):
        return self.targets[w].shape[0] // self.n

    def source(self, w, half, r):
        ref, depth = self.sources[w], self.depth(w)
        part = depth // 2
        cols = self.targets[w].shape[1]
        if ref.shape[0] == depth:
            return ref.at[
                pl.ds(pl.multiple_of(r * part, 16), part),
                pl.ds(pl.multiple_of(half * cols, 128), cols),
            ]
        lower = half * (ref.shape[0] // 2) + self.shifts[w] + r * part
        return ref.at[pl.ds(pl.multiple_of(lower, 16), part), :]

    def piece(self, w, shard, r):
        depth = self.depth(w)
        part = depth // 2
        return self.targets[w].at[pl.ds(pl.multiple_of(shard * depth + r * part, 16), part), :]

    def copy(self, source, target, send_sem, recv_sem, device):
        return pltpu.make_async_remote_copy(
            src_ref=source,
            dst_ref=target,
            send_sem=send_sem,
            recv_sem=recv_sem,
            device_id=device,
            device_id_type=pl.DeviceIdType.MESH,
        )

    def local(self, w, r):
        return pltpu.make_async_copy(
            self.source(w, self.y, r), self.piece(w, self.member(0, 0), r), self.local_sem.at[w, r]
        )

    def half_of(self, i):
        return self.x if i == 0 else 1 - self.x

    def y_copy(self, w, i):
        r = self.half_of(i)
        return self.copy(
            self.source(w, 1 - self.y, r),
            self.piece(w, self.member(0, 0), r),
            self.y_send.at[w, i],
            self.y_recv.at[w, i],
            {"fs": self.member(0, 1)},
        )

    def y_arrival(self, w, i):
        target = self.piece(w, self.member(0, 1), self.half_of(i))
        return self.copy(
            target, target, self.y_send.at[w, i], self.y_recv.at[w, i], {"fs": self.member(0, 1)}
        )

    def hop(self, w, q, k, level):
        shard = self.member(k, q)
        target = self.piece(w, shard, self.x)
        source = self.source(w, self.y, self.x) if k == 0 and q == 0 else target
        step = level - self.level(k)
        lane = step + self.n // 2 - 1
        return self.copy(
            source,
            target,
            self.z_send.at[w, q, lane],
            self.z_recv.at[w, q, lane],
            {"fs": 2 * level + self.y},
        )

    def z_arrival(self, w, q, k):
        target = self.piece(w, self.member(k, q), self.x)
        lane = self.z - self.level(k) + self.n // 2 - 1
        return self.copy(
            target,
            target,
            self.z_send.at[w, q, lane],
            self.z_recv.at[w, q, lane],
            {"fs": self.member(1, 0)},
        )

    def onward(self, w, q, k):
        level = self.level(2) if k == 1 else self.level(1)
        return self.hop(w, q, k, level)

    def x_copy(self, w, q, k):
        target = self.piece(w, self.member(k, q), self.x)
        return self.copy(
            target, target, self.x_send.at[w, q, k], self.x_recv.at[w, q, k], {"rep": 1 - self.x}
        )

    def x_arrival(self, w, q, k):
        target = self.piece(w, self.member(k, q), 1 - self.x)
        return self.copy(
            target, target, self.x_send.at[w, q, k], self.x_recv.at[w, q, k], {"rep": 1 - self.x}
        )

    def end_start(self, w, q):
        @pl.when(jnp.logical_not(self.inner))
        def _():
            self.hop(w, q, 0, self.level(1)).start()

    def inner_start(self, w, q):
        @pl.when(self.inner)
        def _():
            self.hop(w, q, 0, self.level(1)).start()
            self.hop(w, q, 0, self.level(2)).start()

    def z_start(self, w, q):
        self.hop(w, q, 0, self.level(1)).start()

        @pl.when(self.inner)
        def _():
            self.hop(w, q, 0, self.level(2)).start()

    def crossed(self, w):
        self.y_arrival(w, 0).wait_recv()

    def cross(self, w):
        self.crossed(w)
        self.z_start(w, 1)

    def serve(self, w, q, k):
        self.z_arrival(w, q, k).wait_recv()

        @pl.when(self.inner)
        def _():
            self.onward(w, q, k).start()

        self.x_copy(w, q, k).start()

    def split_serve(self, at_end, at_inner):
        @pl.when(self.inner)
        def _():
            w, k, q = at_inner
            self.z_arrival(w, q, k).wait_recv()
            self.onward(w, q, k).start()
            self.x_copy(w, q, k).start()

        @pl.when(jnp.logical_not(self.inner))
        def _():
            w, k, q = at_end
            self.z_arrival(w, q, k).wait_recv()
            self.x_copy(w, q, k).start()

    def own_ready(self, w):
        for r in (0, 1):
            self.local(w, r).wait()
        self.y_arrival(w, 1).wait_recv()

    def ready(self, w):
        self.own_ready(w)
        for q in (0, 1):
            for k in (1, 2, 3):
                self.x_arrival(w, q, k).wait_recv()

    def drain(self, w):
        for i in (0, 1):
            self.y_copy(w, i).wait_send()
        for q in (0, 1):
            self.hop(w, q, 0, self.level(1)).wait_send()
            for k in (1, 2, 3):
                self.x_copy(w, q, k).wait_send()

            @pl.when(self.inner)
            def _():
                self.hop(w, q, 0, self.level(2)).wait_send()
                for k in (1, 2, 3):
                    self.onward(w, q, k).wait_send()


def gelu_of(x):
    return 0.5 * x * (1.0 + jnp.tanh(0.7978845608028654 * (x + 0.044715 * (x * x * x))))


def one_less_exp(z):
    series = 1.0 + z * (1.0 / 6.0)
    for order in (5.0, 4.0, 3.0, 2.0):
        series = 1.0 + z * (1.0 / order) * series
    return jnp.where(z > -0.35, -z * series, 1.0 - jnp.exp(z))


def tap_rows(values, taps_ref, cols):
    extent = taps_ref.shape[0]
    summed = taps_ref[extent - 1 : extent, cols] * values
    row = lax.broadcasted_iota(jnp.int32, values.shape, 0)
    for back in range(1, extent):
        moved = jnp.where(row >= back, pltpu.roll(values, back, 0), 0.0)
        summed = summed + taps_ref[extent - 1 - back : extent - back, cols] * moved
    return summed


def dot32(a, b):
    return jnp.dot(a, b, preferred_element_type=jnp.float32)


def layer_kernel(n, *refs):
    sources = refs[:6] + refs[5:6]
    (stream, reset_map, admit_map, decay_rate, taps, spike) = refs[6:12]
    (gate_taps, value_taps, rec_gain, ffn_gain, last_gain, out) = refs[12:18]
    targets = refs[18:25]
    (whole, spike_in, normed, gate_src, decay, inflow, mixed) = refs[25:32]
    (away, landed, kept, share, share_in, middle, middle_in, gate_up, hidden) = refs[32:41]
    (terms, landed_down, down, down_own, down_in, final, sums, sums_in) = refs[41:49]
    gather_sems = refs[49:56]
    (keep_sem, pair_send, pair_recv, near_send, near_recv, far_send, far_recv) = refs[56:]
    tokens, width = stream.shape
    me = lax.axis_index("tp")
    shifts = [0] * 6 + [targets[5].shape[0] // n]
    gather = PairGather(n, sources, targets, shifts, gather_sems)
    last = len(targets) - 1
    side = gather.y
    bf16, f32 = jnp.bfloat16, jnp.float32
    tile = 256
    strip = 48
    channels = width // 2
    units = hidden.shape[1]
    chunks = 4
    chunk = 2 * tokens // chunks

    def near(i, source, target):
        return gather.copy(source, target, near_send.at[i], near_recv.at[i], {"tp": 1 - me})

    def far(i, source, target):
        return gather.copy(
            source, target, far_send.at[i], far_recv.at[i], {"fs": gather.member(0, 1)}
        )

    def pair(i, source, target):
        return gather.copy(source, target, pair_send.at[i], pair_recv.at[i], {"tp": 1 - me})

    def half(which):
        return pl.ds(pl.multiple_of(which * width, 128), width)

    def strips(lower, upper, body):
        def step(i, carry):
            body(pl.ds(pl.multiple_of(lower + i * strip, 16), strip))
            return carry

        lax.fori_loop(0, (upper - lower) // strip, step, 0)

    def norm_rows(lower, upper, mine, theirs, gain):
        def body(rows):
            a = mine(rows).astype(f32)
            b = theirs(rows).astype(f32)
            total = jnp.sum(a * a, axis=1, keepdims=True) + jnp.sum(b * b, axis=1, keepdims=True)
            inverse = lax.rsqrt(total * (1.0 / (2 * width)) + EPS)
            normed[rows, half(me)] = (a * inverse * gain[:, half(me)]).astype(bf16)
            normed[rows, half(1 - me)] = (b * inverse * gain[:, half(1 - me)]).astype(bf16)

        strips(lower, upper, body)

    first_rows, second_rows = pl.ds(0, tokens), pl.ds(tokens, tokens)
    mine_in = lambda rows: whole[rows, half(me)]
    theirs_in = lambda rows: whole[rows, half(1 - me)]

    arrivals = [(k, q) for k in (1, 2, 3) for q in (0, 1)]
    opening = [(0, 1, 0), (1, 1, 0), (0, 1, 1), (0, 2, 0), (1, 1, 1), (0, 2, 1), (0, 3, 0), (0, 3, 1)]
    inner_opening = [opening[i] for i in (0, 3, 1, 2, 5, 4, 6, 7)]
    steady = []
    for w in range(1, last + 1):
        steady += [(w, 2, 0), (w, 2, 1)]
        for q in (0, 1):
            steady.append((w, 3, q))
            if w < last:
                steady.append((w + 1, 1, q))
    plan, inner_plan = opening + steady, inner_opening + steady
    served = [0]

    def pump(upto):
        while served[0] < upto:
            w, k, q = plan[served[0]]
            if plan[served[0]] == inner_plan[served[0]]:
                gather.serve(w, q, k)
            else:
                gather.split_serve(plan[served[0]], inner_plan[served[0]])
            served[0] += 1
            if 0 < w < last:
                if (k, q) == (1, 1):
                    gather.end_start(w + 1, 0)
                if (k, q) == (2, 1):
                    gather.crossed(w + 1)
                    gather.end_start(w + 1, 1)
                if k == 3:
                    gather.inner_start(w + 1, q)
            if served[0] == 4:
                gather.y_copy(3, 0).start()
                sent_spike.start()
                gather.y_copy(2, 1).start()
            if served[0] == 9:
                gather.y_copy(4, 0).start()
                gather.y_copy(5, 0).start()
                gather.y_copy(6, 0).start()
                gather.y_copy(3, 1).start()

    sent_spike = far(1, spike, spike_in)
    gather.enter()
    own_half = near(0, stream, whole.at[first_rows, half(me)])
    own_half.start()
    gather.y_copy(0, 0).start()
    gather.z_start(0, 0)
    gather.y_copy(1, 0).start()
    gather.y_copy(2, 0).start()
    sent_half = far(0, stream, whole.at[second_rows, half(me)])
    sent_half.start()
    gather.y_copy(0, 1).start()
    gather.y_copy(1, 1).start()
    keep = pltpu.make_async_copy(stream, whole.at[first_rows, half(me)], keep_sem.at[0])
    keep.start()
    gather.z_start(1, 0)
    for w in range(last + 1):
        for r in (0, 1):
            gather.local(w, r).start()
    gather.cross(0)
    pump(2)
    gather.cross(1)
    pump(8)
    keep.wait()
    own_half.wait()
    norm_rows(0, tokens, mine_in, theirs_in, rec_gain)
    pump(10)
    sent_half.wait()
    passed = whole.at[second_rows, half(me)]
    pass_on = near(1, passed, passed)
    pass_on.start()
    pump(11)
    pass_on.wait()
    norm_rows(tokens, 2 * tokens, mine_in, theirs_in, rec_gain)
    pump(16)
    gather.ready(0)
    gather.ready(1)
    sent_spike.wait()

    events_of = [spike[...].T, spike_in[...].T]
    row_sets = [pl.ds(s * tokens, tokens) for s in (0, 1)]
    base = side * channels

    def decay_base(cols):
        rate = -decay_rate[:, cols]
        return GATE_POWER * (jnp.maximum(rate, 0.0) + jnp.log1p(jnp.exp(-jnp.abs(rate))))

    def wide(start, size):
        return pl.ds(pl.multiple_of(start, 128), size)

    for c in range(channels // tile):
        cols = slice(c * tile, (c + 1) * tile)
        for s in (0, 1):
            rows = row_sets[s]
            rec = dot32(normed[rows, :], targets[0][:, cols]).astype(bf16).astype(f32)
            conv = tap_rows(rec, taps, wide(base + c * tile, tile)).astype(bf16)
            gate_src[rows, cols] = dot32(normed[rows, :], targets[1][:, cols]).astype(bf16)
            spikes = events_of[s]
            for part in range(tile // 128):
                h = c * (tile // 128) + part
                heads = channels // 128
                lanes = slice(h * 128, (h + 1) * 128)
                block = conv[:, part * 128 : (part + 1) * 128]
                reset = jax.nn.sigmoid(dot32(block, reset_map[side * heads + h]))
                admit = jax.nn.sigmoid(dot32(block, admit_map[side * heads + h]))
                events = jnp.where(
                    side == 0, spikes[:, h : h + 1], spikes[:, heads + h : heads + h + 1]
                )
                log_decay = events - reset * decay_base(wide(base + h * 128, 128))
                decay[rows, lanes] = jnp.exp(log_decay)
                inflow[rows, lanes] = (
                    jnp.sqrt(one_less_exp(2.0 * log_decay)) * admit * block.astype(f32)
                )
            pump(17 + c * s)

    row = lax.broadcasted_iota(jnp.int32, (8, channels), 0)

    def scan_step(i, carry):
        passed_on = []
        for s in (0, 1):
            rows = pl.ds(pl.multiple_of(s * tokens + i * 16, 16), 16)
            a16, b16 = decay[rows, :], inflow[rows, :]
            state = carry[s]
            found = []
            for part in range(2):
                a, b = a16[part * 8 : part * 8 + 8], b16[part * 8 : part * 8 + 8]
                for back in (1, 2, 4):
                    a_before = jnp.where(row >= back, pltpu.roll(a, back, 0), 1.0)
                    b_before = jnp.where(row >= back, pltpu.roll(b, back, 0), 0.0)
                    b = a * b_before + b
                    a = a * a_before
                states = a * state + b
                state = states[7:8, :]
                found.append(states)
            states = jnp.concatenate(found, axis=0)
            mixed[rows, :] = (states * gelu_of(gate_src[rows, :].astype(f32))).astype(bf16)
            passed_on.append(state)
        return tuple(passed_on)

    still = jnp.zeros((1, channels), f32)
    halfway = tokens // 32
    carry = lax.fori_loop(0, halfway, scan_step, (still, still))
    pump(19)
    lax.fori_loop(halfway, tokens // 16, scan_step, carry)
    gather.ready(2)

    per_half = n // 2
    depth = channels

    def block_of(w, slot, depth):
        return targets[w][pl.ds(pl.multiple_of(slot * depth, 16), depth), :]

    def away_step(j, carry):
        cols = wide(j * tile, tile)
        away[:, cols] = dot32(mixed[...], block_of(2, (1 - me) * per_half + j, depth)).astype(bf16)
        near(2 + j, away.at[:, cols], landed.at[:, cols]).start()
        return carry

    def keep_step(j, carry):
        cols = wide(j * tile, tile)
        kept[:, cols] = dot32(mixed[...], block_of(2, me * per_half + j, depth)).astype(bf16)
        return carry

    lax.fori_loop(0, per_half, away_step, 0)
    lax.fori_loop(0, per_half, keep_step, 0)
    for j in range(per_half):
        cols = slice(j * tile, (j + 1) * tile)
        near(2 + j, away.at[:, cols], landed.at[:, cols]).wait()

    def share_rows(rows):
        share[rows, :] = (kept[rows, :].astype(f32) + landed[rows, :].astype(f32)).astype(bf16)

    def share_copy(i):
        rows = pl.ds((i + chunks // 2) % chunks * chunk, chunk)
        return far(2 + i, share.at[rows, :], share_in.at[pl.ds(i * chunk, chunk), :])

    def middle_copy(i):
        rows = pl.ds(i * chunk, chunk)
        return pair(i, middle.at[rows, :], middle_in.at[rows, :])

    for i in range(chunks):
        lower = (i + chunks // 2) % chunks * chunk
        strips(lower, lower + chunk, share_rows)
        share_copy(i).start()
    for later in (4, 5, 6):
        gather.y_copy(later, 1).start()

    def add_branch(rows):
        branch = (share[rows, :].astype(f32) + share_in[rows, :].astype(f32)).astype(bf16)
        middle[rows, :] = (whole[rows, half(me)].astype(f32) + branch.astype(f32)).astype(bf16)

    for i in range(chunks):
        pump((22, 24, 25, 27)[i])
        share_copy(i).wait()
        strips(i * chunk, (i + 1) * chunk, add_branch)
        middle_copy(i).start()
        pump((23, 25, 26, 27)[i])
        middle_copy(i).wait()
        norm_rows(
            i * chunk,
            (i + 1) * chunk,
            lambda rows: middle[rows, :],
            lambda rows: middle_in[rows, :],
            ffn_gain,
        )
    gather.ready(3)

    unit_base = side * units
    tiles = units // tile

    def gate_step(j, carry):
        cols = wide(j * tile, tile)
        gate_up[:, cols] = dot32(normed[...], targets[3][:, cols]).astype(bf16)
        return carry

    for j in range(tiles):
        lax.fori_loop(j, j + 1, gate_step, 0)
        pump((28, 28, 29, 29)[j])
    pump(35)
    gather.ready(4)

    def up_step(j, carry):
        cols = wide(j * tile, tile)
        for s in (0, 1):
            rows = row_sets[s]
            picked = wide(unit_base + j * tile, tile)
            value = dot32(normed[rows, :], targets[4][:, cols]).astype(bf16).astype(f32)
            value = tap_rows(value, value_taps, picked)
            gate = gelu_of(tap_rows(gate_up[rows, cols].astype(f32), gate_taps, picked))
            hidden[rows, cols] = (gate * value).astype(bf16)
        return carry

    for j in range(tiles):
        lax.fori_loop(j, j + 1, up_step, 0)
        pump((35, 36, 36, 37)[j])

    low = gather.z // 2
    order = [(0, 0), (0, 1)] + arrivals

    def owned(k):
        return (me == low) if k in (0, 1) else (me == 1 - low)

    def slot_of(i):
        k, q = order[i]
        return gather.member(k, q)

    def place_of(i):
        return wide(lax.rem(slot_of(i), per_half) * tile, tile)

    def down_copy(i, s):
        cols = wide(slot_of(i) * tile, tile)
        rows = row_sets[s]
        return near(
            2 + per_half + 2 * i + s, terms.at[rows, cols], landed_down.at[rows, place_of(i)]
        )

    def down_far(i):
        place = place_of(i)
        at = 2 + chunks + lax.rem(slot_of(i), per_half)
        return gather.copy(
            down.at[:, place],
            down_in.at[:, place],
            far_send.at[at],
            far_recv.at[at],
            {"fs": gather.member(0, 1)},
        )

    block_rows = 128

    def blocks(body):
        def step(r, carry):
            body(pl.multiple_of(r * block_rows, 16))
            return carry

        lax.fori_loop(0, tokens // block_rows, step, 0)

    def fold(i):
        @pl.when(owned(order[i][0]))
        def _():
            cols, place = wide(slot_of(i) * tile, tile), place_of(i)

            def folded(lower):
                rows = pl.ds(lower, block_rows)
                return (terms[rows, cols].astype(f32) + landed_down[rows, place].astype(f32)).astype(
                    bf16
                )

            def far_rows(lower):
                down[pl.ds(lower, block_rows), place] = folded(tokens + lower)

            def own_rows(lower):
                down_own[pl.ds(lower, block_rows), place] = folded(lower)

            down_copy(i, 1).wait_recv()
            blocks(far_rows)
            down_far(i).start()
            down_copy(i, 0).wait_recv()
            blocks(own_rows)

    def finish(i):
        @pl.when(owned(order[i][0]))
        def _():
            place = place_of(i)
            down_far(i).wait()

            def body(lower):
                rows = pl.ds(lower, block_rows)
                branch = down_own[rows, place].astype(f32) + down_in[rows, place].astype(f32)
                total = middle[rows, place].astype(f32) + branch.astype(bf16).astype(f32)
                final[rows, place] = total
                square = jnp.sum(total * total, axis=1, keepdims=True)
                before = 0.0 if i in (0, per_half) else sums[rows, :]
                sums[rows, :] = before + jnp.broadcast_to(square, (block_rows, 128))

            blocks(body)

    cut = units // 2
    for i in range(len(order)):
        k, q = order[i]
        if i == 0:
            gather.own_ready(5)
            gather.own_ready(6)
        pump((37, 38, 39, 41, 42, 42, 42, 42)[i])
        if k > 0:
            gather.x_arrival(5, q, k).wait_recv()
            gather.x_arrival(6, q, k).wait_recv()
        cols = wide(slot_of(i) * tile, tile)
        for s in (1, 0):
            rows = row_sets[s]
            first_cut = dot32(hidden[rows, :cut], block_of(5, slot_of(i), cut))
            second_cut = dot32(hidden[rows, cut:], block_of(6, slot_of(i), cut))
            terms[rows, cols] = (first_cut + second_cut).astype(bf16)

            @pl.when(jnp.logical_not(owned(k)))
            def _():
                down_copy(i, s).start()

            if s == 1 and i > 5:
                fold(i - 1)
        if 0 < i < 6:
            fold(i - 1)
    fold(len(order) - 1)
    for i in range(len(order)):
        finish(i)
    for i in range(len(order)):

        @pl.when(jnp.logical_not(owned(order[i][0])))
        def _():
            for s in (0, 1):
                down_copy(i, s).wait_send()

    summed = pair(chunks, sums, sums_in)
    summed.start()
    summed.wait()

    def scale(rows):
        square = sums[rows, :] + sums_in[rows, :]
        inverse = lax.rsqrt(square * (1.0 / (2 * width)) + EPS)[:, 0:1]
        out[rows, :] = (final[rows, :] * inverse * last_gain[:, half(me)]).astype(bf16)

    strips(0, tokens, scale)
    for w in range(last + 1):
        gather.drain(w)


def fused_layer(n, weights, others):
    tokens, width = others[0].shape
    units = weights[3].shape[1] // 2
    channels = width // 2
    bf16, f32 = jnp.bfloat16, jnp.float32
    vmem = pltpu.VMEM
    dma = pltpu.SemaphoreType.DMA
    halves = []
    for w in weights:
        if w.shape[0] == 2 * width // n:
            halves.append((n * w.shape[0], w.shape[1] // 2))
        else:
            halves.append((n * w.shape[0] // 2, w.shape[1]))
    halves[-1:] = [(halves[-1][0] // 2, halves[-1][1])] * 2
    parts = len(halves)
    both = 2 * tokens
    return pl.pallas_call(
        functools.partial(layer_kernel, n),
        out_shape=jax.ShapeDtypeStruct((tokens, width), bf16),
        in_specs=[pl.BlockSpec(memory_space=pl.ANY)] * 6
        + [pl.BlockSpec(memory_space=vmem)] * len(others),
        out_specs=pl.BlockSpec(memory_space=vmem),
        scratch_shapes=[vmem(shape, bf16) for shape in halves]
        + [
            vmem((both, 2 * width), bf16),
            vmem(others[5].shape, f32),
            vmem((both, 2 * width), bf16),
            vmem((both, channels), bf16),
            vmem((both, channels), f32),
            vmem((both, channels), f32),
            vmem((both, channels), bf16),
            vmem((both, width), bf16),
            vmem((both, width), bf16),
            vmem((both, width), bf16),
            vmem((both, width), bf16),
            vmem((both, width), bf16),
            vmem((both, width), bf16),
            vmem((both, width), bf16),
            vmem((both, units), bf16),
            vmem((both, units), bf16),
            vmem((both, 2 * width), bf16),
            vmem((both, width), bf16),
            vmem((tokens, width), bf16),
            vmem((tokens, width), bf16),
            vmem((tokens, width), bf16),
            vmem((tokens, width), f32),
            vmem((tokens, 128), f32),
            vmem((tokens, 128), f32),
            dma((parts, 2)),
            dma((parts, 2)),
            dma((parts, 2)),
            dma((parts, 2, n - 1)),
            dma((parts, 2, n - 1)),
            dma((parts, 2, 4)),
            dma((parts, 2, 4)),
            dma((1,)),
            dma((5,)),
            dma((5,)),
            dma((2 + n // 2 + 2 * n,)),
            dma((2 + n // 2 + 2 * n,)),
            dma((6 + n // 2,)),
            dma((6 + n // 2,)),
        ],
        compiler_params=pltpu.CompilerParams(
            collective_id=0, has_side_effects=True, vmem_limit_bytes=66_000_000
        ),
    )(*weights, *others)


def shards(
    ringed,
    stream,
    recurrence_input_weight,
    output_gate_weight,
    recurrence_gate_matrix,
    input_gate_matrix,
    channel_decay_rate,
    recurrence_taps,
    spike_log_decay,
    recurrence_output_weight,
    feedforward_gate_upward,
    feedforward_value_upward,
    feedforward_gate_taps,
    feedforward_value_taps,
    feedforward_down_weight,
    recurrence_norm_gain,
    feedforward_norm_gain,
    closing_norm_gain,
):
    tok_rows = stream.shape[0]
    fs_size = lax.axis_size("fs")
    if ringed:
        return fused_layer(
            fs_size,
            (
                recurrence_input_weight,
                output_gate_weight,
                recurrence_output_weight,
                feedforward_gate_upward,
                feedforward_value_upward,
                feedforward_down_weight,
            ),
            (
                stream,
                recurrence_gate_matrix,
                input_gate_matrix,
                channel_decay_rate[None, :],
                recurrence_taps,
                spike_log_decay.T,
                feedforward_gate_taps,
                feedforward_value_taps,
                recurrence_norm_gain[None, :],
                feedforward_norm_gain[None, :],
                closing_norm_gain[None, :],
            ),
        )
    weights = [
        lax.all_gather(recurrence_input_weight, "fs", axis=0, tiled=True),
        lax.all_gather(output_gate_weight, "fs", axis=0, tiled=True),
        lax.all_gather(recurrence_output_weight, "fs", axis=1, tiled=True),
        lax.all_gather(feedforward_gate_upward, "fs", axis=0, tiled=True),
        lax.all_gather(feedforward_value_upward, "fs", axis=0, tiled=True),
        lax.all_gather(feedforward_down_weight, "fs", axis=1, tiled=True),
    ]
    head_count = recurrence_gate_matrix.shape[0]
    block_size = recurrence_gate_matrix.shape[1]
    whole_rows = lax.all_gather(stream, "tp", axis=1, tiled=True)
    normed = rms_scale(whole_rows, recurrence_norm_gain)
    rec_sum, gate_sum = fold_pair(
        normed,
        (
            weights[0],
            weights[1],
        ),
    )
    rec_in = rec_sum.astype(jnp.bfloat16)
    gate_src = gate_sum.astype(jnp.bfloat16)
    conv_out = causal_mix(rec_in.astype(jnp.float32), recurrence_taps).astype(jnp.bfloat16)
    blocks = conv_out.reshape(tok_rows, head_count, block_size)
    gate_restart = jax.nn.sigmoid(
        jnp.einsum(
            "thi,hij->thj", blocks, recurrence_gate_matrix, preferred_element_type=jnp.float32
        )
    )
    admit_gate = jax.nn.sigmoid(
        jnp.einsum("thi,hij->thj", blocks, input_gate_matrix, preferred_element_type=jnp.float32)
    )
    decay_base = (GATE_POWER * jax.nn.softplus(-channel_decay_rate)).reshape(head_count, block_size)
    decay_logarithm = -gate_restart * decay_base + spike_log_decay[:, :, None]
    decay_rate = jnp.exp(decay_logarithm)
    inflow = jnp.sqrt(-jnp.expm1(2.0 * decay_logarithm)) * admit_gate * blocks.astype(jnp.float32)
    states = lax.associative_scan(chain_step, (decay_rate, inflow), axis=0)[1]
    mixed_out = (
        states.reshape(tok_rows, head_count * block_size)
        * jax.nn.gelu(gate_src.astype(jnp.float32))
    ).astype(jnp.bfloat16)
    mix_terms = project_with(
        mixed_out, weights[2]
    )
    branch = lax.psum_scatter(
        lax.optimization_barrier(mix_terms).astype(jnp.float32).astype(jnp.bfloat16),
        "tp",
        scatter_dimension=1,
        tiled=True,
    )
    middle = (stream.astype(jnp.float32) + branch.astype(jnp.float32)).astype(jnp.bfloat16)
    whole_middle = lax.all_gather(middle, "tp", axis=1, tiled=True)
    normed_ffn = rms_scale(whole_middle, feedforward_norm_gain)
    gate_sum_ffn, value_sum_ffn = fold_pair(
        normed_ffn,
        (
            weights[3],
            weights[4],
        ),
    )
    gate_up = gate_sum_ffn.astype(jnp.bfloat16)
    value_up = value_sum_ffn.astype(jnp.bfloat16)
    gate_conv = causal_mix(gate_up.astype(jnp.float32), feedforward_gate_taps)
    value_conv = causal_mix(value_up.astype(jnp.float32), feedforward_value_taps)
    hidden = (jax.nn.gelu(gate_conv) * value_conv).astype(jnp.bfloat16)
    down_terms = project_with(
        hidden, weights[5]
    )
    branch_ffn = lax.psum_scatter(
        lax.optimization_barrier(down_terms).astype(jnp.float32).astype(jnp.bfloat16),
        "tp",
        scatter_dimension=1,
        tiled=True,
    )
    final_rows = middle.astype(jnp.float32) + branch_ffn.astype(jnp.float32)
    col_count = final_rows.shape[1]
    square_sum = lax.psum(jnp.sum(final_rows * final_rows, axis=1), "tp")
    inverse = lax.rsqrt(square_sum / (col_count * lax.axis_size("tp")) + EPS)
    gain_part = lax.dynamic_slice_in_dim(
        closing_norm_gain, lax.axis_index("tp") * col_count, col_count
    )
    return (final_rows * inverse[:, None] * gain_part[None, :]).astype(jnp.bfloat16)


def solution(mesh):
    in_specs = (
        P(("rep", "fs"), "tp"),
        P("fs", "tp"),
        P("fs", "tp"),
        P("tp", None, None),
        P("tp", None, None),
        P("tp"),
        P(None, "tp"),
        P(("rep", "fs"), "tp"),
        P("tp", "fs"),
        P("fs", "tp"),
        P("fs", "tp"),
        P(None, "tp"),
        P(None, "tp"),
        P("tp", "fs"),
        P(),
        P(),
        P(),
    )
    out_specs = P(("rep", "fs"), "tp")
    ringed = mesh.shape["rep"] == 2 and mesh.shape["tp"] == 2 and mesh.shape["fs"] == 8
    body = functools.partial(shards, ringed)
    return jax.shard_map(body, mesh=mesh, in_specs=in_specs, out_specs=out_specs, check_vma=False)
```

```python
import functools

import jax
import jax.numpy as jnp
from jax import lax
from jax.experimental import pallas as pl
from jax.experimental.pallas import tpu as pltpu
from jax.sharding import PartitionSpec as P

EPS = 1e-06
GATE_POWER = 8.0


def rms_scale(row_block, gain_vec):
    widened = row_block.astype(jnp.float32)
    inverse = lax.rsqrt(jnp.mean(widened * widened, axis=-1, keepdims=True) + EPS)
    return (widened * inverse * gain_vec).astype(jnp.bfloat16)


def causal_mix(values, kernel_taps):
    extent = kernel_taps.shape[0]
    length = values.shape[0]
    padded = jnp.pad(values, ((extent - 1, 0), (0, 0)))
    summed = kernel_taps[0] * padded[0:length]
    for offset in range(1, extent):
        summed = summed + kernel_taps[offset] * padded[offset : offset + length]
    return summed


def chain_step(earlier, following):
    return (earlier[0] * following[0], following[0] * earlier[1] + following[1])


def fold_pair(source, pieces):
    return (
        jnp.dot(source, pieces[0], preferred_element_type=jnp.float32),
        jnp.dot(source, pieces[1], preferred_element_type=jnp.float32),
    )


def project_with(left_rows, weight_piece):
    return jnp.dot(left_rows, weight_piece, preferred_element_type=jnp.float32).astype(jnp.bfloat16)


class PairGather:
    def __init__(self, n, sources, targets, shifts, sems):
        self.n = n
        self.shifts = shifts
        self.sources = sources
        self.targets = targets
        (self.local_sem, self.y_send, self.y_recv, self.z_send, self.z_recv, self.x_send, self.x_recv) = sems
        self.x = lax.axis_index("rep")
        fs = lax.axis_index("fs")
        self.y = lax.rem(fs, 2)
        self.z = fs // 2
        levels = n // 2
        self.middle = self.z * (levels - 1 - self.z) // (levels - 2)
        self.inner = self.middle == 1

    def level(self, k):
        levels = self.n // 2
        across = levels - 1 - self.z
        beyond = lax.rem(self.z + levels // 2, levels)
        if k == 0:
            return self.z
        if k == 1:
            return self.z + 1 - 2 * lax.rem(self.z, 2)
        if k == 2:
            return self.middle * across + (1 - self.middle) * beyond
        return self.middle * beyond + (1 - self.middle) * across

    def side(self, q):
        return lax.rem(self.y + q, 2)

    def member(self, k, q):
        return 2 * self.level(k) + self.side(q)

    def enter(self):
        barrier = pltpu.get_barrier_semaphore()
        devices = [
            {"rep": 1 - self.x},
            {"tp": 1 - lax.axis_index("tp")},
            {"fs": self.member(0, 1)},
            {"fs": self.member(1, 0)},
        ]
        for device in devices:
            pl.semaphore_signal(
                barrier, inc=1, device_id=device, device_id_type=pl.DeviceIdType.MESH
            )

        @pl.when(self.inner)
        def _():
            pl.semaphore_signal(
                barrier,
                inc=1,
                device_id={"fs": self.member(2, 0)},
                device_id_type=pl.DeviceIdType.MESH,
            )

        pl.semaphore_wait(barrier, len(devices) + self.middle)

    def depth(self, w):
        return self.targets[w].shape[0] // self.n

    def source(self, w, half, r):
        ref, depth = self.sources[w], self.depth(w)
        part = depth // 2
        cols = self.targets[w].shape[1]
        if ref.shape[0] == depth:
            lower = half * (ref.shape[1] // 2) + self.shifts[w]
            return ref.at[
                pl.ds(pl.multiple_of(r * part, 16), part),
                pl.ds(pl.multiple_of(lower, 128), cols),
            ]
        lower = half * (ref.shape[0] // 2) + self.shifts[w] + r * part
        return ref.at[pl.ds(pl.multiple_of(lower, 16), part), :]

    def piece(self, w, shard, r):
        depth = self.depth(w)
        part = depth // 2
        return self.targets[w].at[pl.ds(pl.multiple_of(shard * depth + r * part, 16), part), :]

    def copy(self, source, target, send_sem, recv_sem, device):
        return pltpu.make_async_remote_copy(
            src_ref=source,
            dst_ref=target,
            send_sem=send_sem,
            recv_sem=recv_sem,
            device_id=device,
            device_id_type=pl.DeviceIdType.MESH,
        )

    def local(self, w, r):
        return pltpu.make_async_copy(
            self.source(w, self.y, r), self.piece(w, self.member(0, 0), r), self.local_sem.at[w, r]
        )

    def half_of(self, i):
        return self.x if i == 0 else 1 - self.x

    def y_copy(self, w, i):
        r = self.half_of(i)
        return self.copy(
            self.source(w, 1 - self.y, r),
            self.piece(w, self.member(0, 0), r),
            self.y_send.at[w, i],
            self.y_recv.at[w, i],
            {"fs": self.member(0, 1)},
        )

    def y_arrival(self, w, i):
        target = self.piece(w, self.member(0, 1), self.half_of(i))
        return self.copy(
            target, target, self.y_send.at[w, i], self.y_recv.at[w, i], {"fs": self.member(0, 1)}
        )

    def hop(self, w, q, k, level):
        shard = self.member(k, q)
        target = self.piece(w, shard, self.x)
        source = self.source(w, self.y, self.x) if k == 0 and q == 0 else target
        step = level - self.level(k)
        lane = step + self.n // 2 - 1
        return self.copy(
            source,
            target,
            self.z_send.at[w, q, lane],
            self.z_recv.at[w, q, lane],
            {"fs": 2 * level + self.y},
        )

    def z_arrival(self, w, q, k):
        target = self.piece(w, self.member(k, q), self.x)
        lane = self.z - self.level(k) + self.n // 2 - 1
        return self.copy(
            target,
            target,
            self.z_send.at[w, q, lane],
            self.z_recv.at[w, q, lane],
            {"fs": self.member(1, 0)},
        )

    def onward(self, w, q, k):
        level = self.level(2) if k == 1 else self.level(1)
        return self.hop(w, q, k, level)

    def x_copy(self, w, q, k):
        target = self.piece(w, self.member(k, q), self.x)
        return self.copy(
            target, target, self.x_send.at[w, q, k], self.x_recv.at[w, q, k], {"rep": 1 - self.x}
        )

    def x_arrival(self, w, q, k):
        target = self.piece(w, self.member(k, q), 1 - self.x)
        return self.copy(
            target, target, self.x_send.at[w, q, k], self.x_recv.at[w, q, k], {"rep": 1 - self.x}
        )

    def end_start(self, w, q):
        @pl.when(jnp.logical_not(self.inner))
        def _():
            self.hop(w, q, 0, self.level(1)).start()

    def inner_start(self, w, q):
        @pl.when(self.inner)
        def _():
            self.hop(w, q, 0, self.level(1)).start()
            self.hop(w, q, 0, self.level(2)).start()

    def z_start(self, w, q):
        self.hop(w, q, 0, self.level(1)).start()

        @pl.when(self.inner)
        def _():
            self.hop(w, q, 0, self.level(2)).start()

    def edge_start(self, w, q):
        self.hop(w, q, 0, self.level(1)).start()

    def core_start(self, w, q):
        @pl.when(self.inner)
        def _():
            self.hop(w, q, 0, self.level(2)).start()

    def crossed(self, w):
        self.y_arrival(w, 0).wait_recv()

    def cross(self, w):
        self.crossed(w)
        self.z_start(w, 1)

    def serve(self, w, q, k):
        self.z_arrival(w, q, k).wait_recv()

        @pl.when(self.inner)
        def _():
            self.onward(w, q, k).start()

        self.x_copy(w, q, k).start()

    def split_serve(self, at_end, at_inner):
        @pl.when(self.inner)
        def _():
            w, k, q = at_inner
            self.z_arrival(w, q, k).wait_recv()
            self.onward(w, q, k).start()
            self.x_copy(w, q, k).start()

        @pl.when(jnp.logical_not(self.inner))
        def _():
            w, k, q = at_end
            self.z_arrival(w, q, k).wait_recv()
            self.x_copy(w, q, k).start()

    def own_ready(self, w):
        for r in (0, 1):
            self.local(w, r).wait()
        self.y_arrival(w, 1).wait_recv()

    def ready(self, w):
        self.own_ready(w)
        for q in (0, 1):
            for k in (1, 2, 3):
                self.x_arrival(w, q, k).wait_recv()

    def drain(self, w):
        for i in (0, 1):
            self.y_copy(w, i).wait_send()
        for q in (0, 1):
            self.hop(w, q, 0, self.level(1)).wait_send()
            for k in (1, 2, 3):
                self.x_copy(w, q, k).wait_send()

            @pl.when(self.inner)
            def _():
                self.hop(w, q, 0, self.level(2)).wait_send()
                for k in (1, 2, 3):
                    self.onward(w, q, k).wait_send()


def gelu_of(x):
    return 0.5 * x * (1.0 + jnp.tanh(0.7978845608028654 * (x + 0.044715 * (x * x * x))))


def one_less_exp(z):
    series = 1.0 + z * (1.0 / 6.0)
    for order in (5.0, 4.0, 3.0, 2.0):
        series = 1.0 + z * (1.0 / order) * series
    return jnp.where(z > -0.35, -z * series, 1.0 - jnp.exp(z))


def tap_rows(values, taps_ref, cols):
    extent = taps_ref.shape[0]
    summed = taps_ref[extent - 1 : extent, cols] * values
    row = lax.broadcasted_iota(jnp.int32, values.shape, 0)
    for back in range(1, extent):
        moved = jnp.where(row >= back, pltpu.roll(values, back, 0), 0.0)
        summed = summed + taps_ref[extent - 1 - back : extent - back, cols] * moved
    return summed


def dot32(a, b):
    return jnp.dot(a, b, preferred_element_type=jnp.float32)


def layer_kernel(n, *refs):
    sources = [refs[i] for i in (0, 1, 2, 3, 3, 4, 4, 5, 5)]
    (stream, reset_map, admit_map, decay_rate, taps, spike) = refs[6:12]
    (gate_taps, value_taps, rec_gain, ffn_gain, last_gain, out) = refs[12:18]
    targets = refs[18:27]
    (whole, spike_in, normed, gate_src, decay, inflow, mixed) = refs[27:34]
    (away, landed, kept, share, share_in, middle, middle_in, gate_up, hidden) = refs[34:43]
    (terms, landed_down, down, down_own, down_in, final, sums, sums_in) = refs[43:51]
    gather_sems = refs[51:58]
    (keep_sem, pair_send, pair_recv, near_send, near_recv, far_send, far_recv) = refs[58:]
    tokens, width = stream.shape
    me = lax.axis_index("tp")
    wide_cut, deep_cut = targets[3].shape[1], targets[7].shape[0] // n
    shifts = [0, 0, 0, 0, wide_cut, 0, wide_cut, 0, deep_cut]
    gather = PairGather(n, sources, targets, shifts, gather_sems)
    last = len(targets) - 1
    side = gather.y
    bf16, f32 = jnp.bfloat16, jnp.float32
    tile = 256
    strip = 48
    channels = width // 2
    units = hidden.shape[1]
    chunks = 4
    chunk = 2 * tokens // chunks

    def near(i, source, target):
        return gather.copy(source, target, near_send.at[i], near_recv.at[i], {"tp": 1 - me})

    def far(i, source, target):
        return gather.copy(
            source, target, far_send.at[i], far_recv.at[i], {"fs": gather.member(0, 1)}
        )

    def pair(i, source, target):
        return gather.copy(source, target, pair_send.at[i], pair_recv.at[i], {"tp": 1 - me})

    def half(which):
        return pl.ds(pl.multiple_of(which * width, 128), width)

    def strips(lower, upper, body):
        def step(i, carry):
            body(pl.ds(pl.multiple_of(lower + i * strip, 16), strip))
            return carry

        lax.fori_loop(0, (upper - lower) // strip, step, 0)

    def norm_rows(lower, upper, mine, theirs, gain):
        def body(rows):
            a = mine(rows).astype(f32)
            b = theirs(rows).astype(f32)
            total = jnp.sum(a * a, axis=1, keepdims=True) + jnp.sum(b * b, axis=1, keepdims=True)
            inverse = lax.rsqrt(total * (1.0 / (2 * width)) + EPS)
            normed[rows, half(me)] = (a * inverse * gain[:, half(me)]).astype(bf16)
            normed[rows, half(1 - me)] = (b * inverse * gain[:, half(1 - me)]).astype(bf16)

        strips(lower, upper, body)

    first_rows, second_rows = pl.ds(0, tokens), pl.ds(tokens, tokens)
    mine_in = lambda rows: whole[rows, half(me)]
    theirs_in = lambda rows: whole[rows, half(1 - me)]

    arrivals = [(k, q) for k in (1, 2, 3) for q in (0, 1)]
    opening = [(0, 1, 0), (1, 1, 0), (0, 1, 1), (0, 2, 0), (1, 1, 1), (0, 2, 1), (0, 3, 0), (0, 3, 1)]
    inner_opening = [opening[i] for i in (0, 3, 2, 5, 1, 4, 6, 7)]
    steady = []
    for w in range(1, last + 1):
        steady += [(w, 2, 0), (w, 2, 1)]
        for q in (0, 1):
            steady.append((w, 3, q))
            if w < last:
                steady.append((w + 1, 1, q))
    plan, inner_plan = opening + steady, inner_opening + steady
    served = [0]

    def pump(upto):
        while served[0] < upto:
            w, k, q = plan[served[0]]
            if plan[served[0]] == inner_plan[served[0]]:
                gather.serve(w, q, k)
            else:
                gather.split_serve(plan[served[0]], inner_plan[served[0]])
            served[0] += 1
            if 0 < w < last:
                if (k, q) == (1, 1):
                    gather.end_start(w + 1, 0)
                if (k, q) == (2, 1):
                    gather.crossed(w + 1)
                    gather.end_start(w + 1, 1)
                if k == 3:
                    gather.inner_start(w + 1, q)
            if served[0] == 4:
                gather.y_copy(3, 0).start()
                sent_spike.start()
                gather.y_copy(2, 1).start()
                gather.y_copy(4, 0).start()
            if served[0] == 9:
                for later in (5, 6, 7, 8):
                    gather.y_copy(later, 0).start()
                for later in (3, 4):
                    gather.y_copy(later, 1).start()

    sent_spike = far(1, spike, spike_in)
    gather.enter()
    own_half = near(0, stream, whole.at[first_rows, half(me)])
    own_half.start()
    gather.y_copy(0, 0).start()
    gather.z_start(0, 0)
    gather.y_copy(1, 0).start()
    gather.y_copy(2, 0).start()
    sent_half = far(0, stream, whole.at[second_rows, half(me)])
    sent_half.start()
    gather.y_copy(0, 1).start()
    gather.y_copy(1, 1).start()
    keep = pltpu.make_async_copy(stream, whole.at[first_rows, half(me)], keep_sem.at[0])
    keep.start()
    gather.edge_start(1, 0)
    for w in range(last + 1):
        for r in (0, 1):
            gather.local(w, r).start()
    gather.cross(0)
    pump(2)
    gather.core_start(1, 0)
    gather.cross(1)
    pump(8)
    keep.wait()
    own_half.wait()
    norm_rows(0, tokens, mine_in, theirs_in, rec_gain)
    pump(10)
    sent_half.wait()
    passed = whole.at[second_rows, half(me)]
    pass_on = near(1, passed, passed)
    pass_on.start()
    pump(11)
    pass_on.wait()
    norm_rows(tokens, 2 * tokens, mine_in, theirs_in, rec_gain)
    pump(16)
    gather.ready(0)
    gather.ready(1)
    sent_spike.wait()

    events_of = [spike[...].T, spike_in[...].T]
    row_sets = [pl.ds(s * tokens, tokens) for s in (0, 1)]
    base = side * channels

    def decay_base(cols):
        rate = -decay_rate[:, cols]
        return GATE_POWER * (jnp.maximum(rate, 0.0) + jnp.log1p(jnp.exp(-jnp.abs(rate))))

    def wide(start, size):
        return pl.ds(pl.multiple_of(start, 128), size)

    for c in range(channels // tile):
        cols = slice(c * tile, (c + 1) * tile)
        for s in (0, 1):
            rows = row_sets[s]
            rec = dot32(normed[rows, :], targets[0][:, cols]).astype(bf16).astype(f32)
            conv = tap_rows(rec, taps, wide(base + c * tile, tile)).astype(bf16)
            gate_src[rows, cols] = dot32(normed[rows, :], targets[1][:, cols]).astype(bf16)
            spikes = events_of[s]
            for part in range(tile // 128):
                h = c * (tile // 128) + part
                heads = channels // 128
                lanes = slice(h * 128, (h + 1) * 128)
                block = conv[:, part * 128 : (part + 1) * 128]
                reset = jax.nn.sigmoid(dot32(block, reset_map[side * heads + h]))
                admit = jax.nn.sigmoid(dot32(block, admit_map[side * heads + h]))
                events = jnp.where(
                    side == 0, spikes[:, h : h + 1], spikes[:, heads + h : heads + h + 1]
                )
                log_decay = events - reset * decay_base(wide(base + h * 128, 128))
                decay[rows, lanes] = jnp.exp(log_decay)
                inflow[rows, lanes] = (
                    jnp.sqrt(one_less_exp(2.0 * log_decay)) * admit * block.astype(f32)
                )
            pump(17 + c)

    row = lax.broadcasted_iota(jnp.int32, (8, channels), 0)

    def scan_step(i, carry):
        passed_on = []
        for s in (0, 1):
            rows = pl.ds(pl.multiple_of(s * tokens + i * 16, 16), 16)
            a16, b16 = decay[rows, :], inflow[rows, :]
            state = carry[s]
            found = []
            for part in range(2):
                a, b = a16[part * 8 : part * 8 + 8], b16[part * 8 : part * 8 + 8]
                for back in (1, 2, 4):
                    a_before = jnp.where(row >= back, pltpu.roll(a, back, 0), 1.0)
                    b_before = jnp.where(row >= back, pltpu.roll(b, back, 0), 0.0)
                    b = a * b_before + b
                    a = a * a_before
                states = a * state + b
                state = states[7:8, :]
                found.append(states)
            states = jnp.concatenate(found, axis=0)
            mixed[rows, :] = (states * gelu_of(gate_src[rows, :].astype(f32))).astype(bf16)
            passed_on.append(state)
        return tuple(passed_on)

    still = jnp.zeros((1, channels), f32)
    halfway = tokens // 32
    carry = lax.fori_loop(0, halfway, scan_step, (still, still))
    pump(19)
    lax.fori_loop(halfway, tokens // 16, scan_step, carry)
    pump(20)
    gather.ready(2)

    per_half = n // 2
    depth = channels

    def block_of(w, slot, depth):
        return targets[w][pl.ds(pl.multiple_of(slot * depth, 16), depth), :]

    def away_step(j, carry):
        cols = wide(j * tile, tile)
        away[:, cols] = dot32(mixed[...], block_of(2, (1 - me) * per_half + j, depth)).astype(bf16)
        near(2 + j, away.at[:, cols], landed.at[:, cols]).start()
        return carry

    def keep_step(j, carry):
        cols = wide(j * tile, tile)
        kept[:, cols] = dot32(mixed[...], block_of(2, me * per_half + j, depth)).astype(bf16)
        return carry

    lax.fori_loop(0, per_half, away_step, 0)
    pump(21)
    lax.fori_loop(0, per_half, keep_step, 0)
    pump(22)
    for j in range(per_half):
        cols = slice(j * tile, (j + 1) * tile)
        near(2 + j, away.at[:, cols], landed.at[:, cols]).wait()

    def share_rows(rows):
        share[rows, :] = (kept[rows, :].astype(f32) + landed[rows, :].astype(f32)).astype(bf16)

    def share_copy(i):
        rows = pl.ds((i + chunks // 2) % chunks * chunk, chunk)
        return far(2 + i, share.at[rows, :], share_in.at[pl.ds(i * chunk, chunk), :])

    def middle_copy(i):
        rows = pl.ds(i * chunk, chunk)
        return pair(i, middle.at[rows, :], middle_in.at[rows, :])

    for i in range(chunks):
        lower = (i + chunks // 2) % chunks * chunk
        strips(lower, lower + chunk, share_rows)
        share_copy(i).start()
    for later in (5, 6, 7, 8):
        gather.y_copy(later, 1).start()

    def add_branch(rows):
        branch = (share[rows, :].astype(f32) + share_in[rows, :].astype(f32)).astype(bf16)
        middle[rows, :] = (whole[rows, half(me)].astype(f32) + branch.astype(f32)).astype(bf16)

    for i in range(chunks):
        pump((26, 29, 32, 35)[i])
        share_copy(i).wait()
        strips(i * chunk, (i + 1) * chunk, add_branch)
        middle_copy(i).start()
        pump((27, 30, 33, 36)[i])
        middle_copy(i).wait()
        norm_rows(
            i * chunk,
            (i + 1) * chunk,
            lambda rows: middle[rows, :],
            lambda rows: middle_in[rows, :],
            ffn_gain,
        )
    gather.ready(3)
    gather.ready(4)

    unit_base = side * units
    tiles = units // tile
    per_cut = wide_cut // tile

    def gate_step(j):
        inside = slice(j % per_cut * tile, (j % per_cut + 1) * tile)
        block = targets[3 + j // per_cut][:, inside]
        gate_up[:, j * tile : (j + 1) * tile] = dot32(normed[...], block).astype(bf16)

    def up_step(j):
        cols = slice(j * tile, (j + 1) * tile)
        inside = slice(j % per_cut * tile, (j % per_cut + 1) * tile)
        picked = wide(unit_base + j * tile, tile)
        for s in (0, 1):
            rows = row_sets[s]
            block = targets[5 + j // per_cut][:, inside]
            value = dot32(normed[rows, :], block).astype(bf16).astype(f32)
            value = tap_rows(value, value_taps, picked)
            gate = gelu_of(tap_rows(gate_up[rows, cols].astype(f32), gate_taps, picked))
            hidden[rows, cols] = (gate * value).astype(bf16)

    for j in range(tiles):
        gate_step(j)
        pump((37, 38, 38, 39)[j])
    gather.ready(5)
    for j in range(tiles):
        if j == per_cut:
            pump(45)
            gather.ready(6)
        up_step(j)
        pump((40, 41, 46, 47)[j])

    low = gather.z // 2
    order = [(0, 0), (0, 1)] + arrivals

    def owned(k):
        return (me == low) if k in (0, 1) else (me == 1 - low)

    def slot_of(i):
        k, q = order[i]
        return gather.member(k, q)

    def place_of(i):
        return wide(lax.rem(slot_of(i), per_half) * tile, tile)

    def down_copy(i, s):
        cols = wide(slot_of(i) * tile, tile)
        rows = row_sets[s]
        return near(
            2 + per_half + 2 * i + s, terms.at[rows, cols], landed_down.at[rows, place_of(i)]
        )

    def down_far(i):
        place = place_of(i)
        at = 2 + chunks + lax.rem(slot_of(i), per_half)
        return gather.copy(
            down.at[:, place],
            down_in.at[:, place],
            far_send.at[at],
            far_recv.at[at],
            {"fs": gather.member(0, 1)},
        )

    block_rows = 128

    def blocks(body):
        def step(r, carry):
            body(pl.multiple_of(r * block_rows, 16))
            return carry

        lax.fori_loop(0, tokens // block_rows, step, 0)

    def fold(i, s):
        @pl.when(owned(order[i][0]))
        def _():
            cols, place = wide(slot_of(i) * tile, tile), place_of(i)

            def folded(lower):
                rows = pl.ds(lower, block_rows)
                return (terms[rows, cols].astype(f32) + landed_down[rows, place].astype(f32)).astype(
                    bf16
                )

            def far_rows(lower):
                down[pl.ds(lower, block_rows), place] = folded(tokens + lower)

            def own_rows(lower):
                down_own[pl.ds(lower, block_rows), place] = folded(lower)

            if s == 1:
                down_copy(i, 1).wait_recv()
                blocks(far_rows)
                down_far(i).start()
            else:
                down_copy(i, 0).wait_recv()
                blocks(own_rows)

    def finish(i):
        @pl.when(owned(order[i][0]))
        def _():
            place = place_of(i)
            down_far(i).wait()

            def body(lower):
                rows = pl.ds(lower, block_rows)
                branch = down_own[rows, place].astype(f32) + down_in[rows, place].astype(f32)
                total = middle[rows, place].astype(f32) + branch.astype(bf16).astype(f32)
                final[rows, place] = total * last_gain[:, wide(me * width + place.start, tile)]
                square = jnp.sum(total * total, axis=1, keepdims=True)
                before = 0.0 if i in (0, per_half) else sums[rows, :]
                sums[rows, :] = before + jnp.broadcast_to(square, (block_rows, 128))

            blocks(body)

    cut = units // 2
    for i in range(len(order)):
        k, q = order[i]
        if i == 0:
            gather.own_ready(7)
            gather.own_ready(8)
        pump((48, 49, 50, 52, 53, 54, 54, 54)[i])
        if k > 0:
            gather.x_arrival(7, q, k).wait_recv()
            gather.x_arrival(8, q, k).wait_recv()
        cols = wide(slot_of(i) * tile, tile)
        for s in (1, 0):
            rows = row_sets[s]
            first_cut = dot32(hidden[rows, :cut], block_of(7, slot_of(i), cut))
            second_cut = dot32(hidden[rows, cut:], block_of(8, slot_of(i), cut))
            terms[rows, cols] = (first_cut + second_cut).astype(bf16)

            @pl.when(jnp.logical_not(owned(k)))
            def _():
                down_copy(i, s).start()

            if i > 0:
                fold(i - 1, s)
    for s in (1, 0):
        fold(len(order) - 1, s)
    for i in range(len(order)):
        finish(i)
    for i in range(len(order)):

        @pl.when(jnp.logical_not(owned(order[i][0])))
        def _():
            for s in (0, 1):
                down_copy(i, s).wait_send()

    summed = pair(chunks, sums, sums_in)
    summed.start()
    summed.wait()

    def scale(lower):
        rows = pl.ds(lower, block_rows)
        square = sums[rows, :] + sums_in[rows, :]
        inverse = lax.rsqrt(square * (1.0 / (2 * width)) + EPS)[:, 0:1]
        out[rows, :] = (final[rows, :] * inverse).astype(bf16)

    blocks(scale)
    for w in range(last + 1):
        gather.drain(w)


def fused_layer(n, weights, others):
    tokens, width = others[0].shape
    units = weights[3].shape[1] // 2
    channels = width // 2
    bf16, f32 = jnp.bfloat16, jnp.float32
    vmem = pltpu.VMEM
    dma = pltpu.SemaphoreType.DMA
    halves = []
    for w in weights:
        if w.shape[0] == 2 * width // n:
            halves.append((n * w.shape[0], w.shape[1] // 2))
        else:
            halves.append((n * w.shape[0] // 2, w.shape[1]))
    split = [(rows, cols // 2) for rows, cols in halves[3:5] for _ in (0, 1)]
    halves = halves[:3] + split + [(halves[5][0] // 2, halves[5][1])] * 2
    parts = len(halves)
    both = 2 * tokens
    return pl.pallas_call(
        functools.partial(layer_kernel, n),
        out_shape=jax.ShapeDtypeStruct((tokens, width), bf16),
        in_specs=[pl.BlockSpec(memory_space=pl.ANY)] * 6
        + [pl.BlockSpec(memory_space=vmem)] * len(others),
        out_specs=pl.BlockSpec(memory_space=vmem),
        scratch_shapes=[vmem(shape, bf16) for shape in halves]
        + [
            vmem((both, 2 * width), bf16),
            vmem(others[5].shape, f32),
            vmem((both, 2 * width), bf16),
            vmem((both, channels), bf16),
            vmem((both, channels), f32),
            vmem((both, channels), f32),
            vmem((both, channels), bf16),
            vmem((both, width), bf16),
            vmem((both, width), bf16),
            vmem((both, width), bf16),
            vmem((both, width), bf16),
            vmem((both, width), bf16),
            vmem((both, width), bf16),
            vmem((both, width), bf16),
            vmem((both, units), bf16),
            vmem((both, units), bf16),
            vmem((both, 2 * width), bf16),
            vmem((both, width), bf16),
            vmem((tokens, width), bf16),
            vmem((tokens, width), bf16),
            vmem((tokens, width), bf16),
            vmem((tokens, width), f32),
            vmem((tokens, 128), f32),
            vmem((tokens, 128), f32),
            dma((parts, 2)),
            dma((parts, 2)),
            dma((parts, 2)),
            dma((parts, 2, n - 1)),
            dma((parts, 2, n - 1)),
            dma((parts, 2, 4)),
            dma((parts, 2, 4)),
            dma((1,)),
            dma((5,)),
            dma((5,)),
            dma((2 + n // 2 + 2 * n,)),
            dma((2 + n // 2 + 2 * n,)),
            dma((6 + n // 2,)),
            dma((6 + n // 2,)),
        ],
        compiler_params=pltpu.CompilerParams(
            collective_id=0, has_side_effects=True, vmem_limit_bytes=66_000_000
        ),
    )(*weights, *others)


def shards(
    ringed,
    stream,
    recurrence_input_weight,
    output_gate_weight,
    recurrence_gate_matrix,
    input_gate_matrix,
    channel_decay_rate,
    recurrence_taps,
    spike_log_decay,
    recurrence_output_weight,
    feedforward_gate_upward,
    feedforward_value_upward,
    feedforward_gate_taps,
    feedforward_value_taps,
    feedforward_down_weight,
    recurrence_norm_gain,
    feedforward_norm_gain,
    closing_norm_gain,
):
    tok_rows = stream.shape[0]
    fs_size = lax.axis_size("fs")
    if ringed:
        return fused_layer(
            fs_size,
            (
                recurrence_input_weight,
                output_gate_weight,
                recurrence_output_weight,
                feedforward_gate_upward,
                feedforward_value_upward,
                feedforward_down_weight,
            ),
            (
                stream,
                recurrence_gate_matrix,
                input_gate_matrix,
                channel_decay_rate[None, :],
                recurrence_taps,
                spike_log_decay.T,
                feedforward_gate_taps,
                feedforward_value_taps,
                recurrence_norm_gain[None, :],
                feedforward_norm_gain[None, :],
                closing_norm_gain[None, :],
            ),
        )
    weights = [
        lax.all_gather(recurrence_input_weight, "fs", axis=0, tiled=True),
        lax.all_gather(output_gate_weight, "fs", axis=0, tiled=True),
        lax.all_gather(recurrence_output_weight, "fs", axis=1, tiled=True),
        lax.all_gather(feedforward_gate_upward, "fs", axis=0, tiled=True),
        lax.all_gather(feedforward_value_upward, "fs", axis=0, tiled=True),
        lax.all_gather(feedforward_down_weight, "fs", axis=1, tiled=True),
    ]
    head_count = recurrence_gate_matrix.shape[0]
    block_size = recurrence_gate_matrix.shape[1]
    whole_rows = lax.all_gather(stream, "tp", axis=1, tiled=True)
    normed = rms_scale(whole_rows, recurrence_norm_gain)
    rec_sum, gate_sum = fold_pair(
        normed,
        (
            weights[0],
            weights[1],
        ),
    )
    rec_in = rec_sum.astype(jnp.bfloat16)
    gate_src = gate_sum.astype(jnp.bfloat16)
    conv_out = causal_mix(rec_in.astype(jnp.float32), recurrence_taps).astype(jnp.bfloat16)
    blocks = conv_out.reshape(tok_rows, head_count, block_size)
    gate_restart = jax.nn.sigmoid(
        jnp.einsum(
            "thi,hij->thj", blocks, recurrence_gate_matrix, preferred_element_type=jnp.float32
        )
    )
    admit_gate = jax.nn.sigmoid(
        jnp.einsum("thi,hij->thj", blocks, input_gate_matrix, preferred_element_type=jnp.float32)
    )
    decay_base = (GATE_POWER * jax.nn.softplus(-channel_decay_rate)).reshape(head_count, block_size)
    decay_logarithm = -gate_restart * decay_base + spike_log_decay[:, :, None]
    decay_rate = jnp.exp(decay_logarithm)
    inflow = jnp.sqrt(-jnp.expm1(2.0 * decay_logarithm)) * admit_gate * blocks.astype(jnp.float32)
    states = lax.associative_scan(chain_step, (decay_rate, inflow), axis=0)[1]
    mixed_out = (
        states.reshape(tok_rows, head_count * block_size)
        * jax.nn.gelu(gate_src.astype(jnp.float32))
    ).astype(jnp.bfloat16)
    mix_terms = project_with(
        mixed_out, weights[2]
    )
    branch = lax.psum_scatter(
        lax.optimization_barrier(mix_terms).astype(jnp.float32).astype(jnp.bfloat16),
        "tp",
        scatter_dimension=1,
        tiled=True,
    )
    middle = (stream.astype(jnp.float32) + branch.astype(jnp.float32)).astype(jnp.bfloat16)
    whole_middle = lax.all_gather(middle, "tp", axis=1, tiled=True)
    normed_ffn = rms_scale(whole_middle, feedforward_norm_gain)
    gate_sum_ffn, value_sum_ffn = fold_pair(
        normed_ffn,
        (
            weights[3],
            weights[4],
        ),
    )
    gate_up = gate_sum_ffn.astype(jnp.bfloat16)
    value_up = value_sum_ffn.astype(jnp.bfloat16)
    gate_conv = causal_mix(gate_up.astype(jnp.float32), feedforward_gate_taps)
    value_conv = causal_mix(value_up.astype(jnp.float32), feedforward_value_taps)
    hidden = (jax.nn.gelu(gate_conv) * value_conv).astype(jnp.bfloat16)
    down_terms = project_with(
        hidden, weights[5]
    )
    branch_ffn = lax.psum_scatter(
        lax.optimization_barrier(down_terms).astype(jnp.float32).astype(jnp.bfloat16),
        "tp",
        scatter_dimension=1,
        tiled=True,
    )
    final_rows = middle.astype(jnp.float32) + branch_ffn.astype(jnp.float32)
    col_count = final_rows.shape[1]
    square_sum = lax.psum(jnp.sum(final_rows * final_rows, axis=1), "tp")
    inverse = lax.rsqrt(square_sum / (col_count * lax.axis_size("tp")) + EPS)
    gain_part = lax.dynamic_slice_in_dim(
        closing_norm_gain, lax.axis_index("tp") * col_count, col_count
    )
    return (final_rows * inverse[:, None] * gain_part[None, :]).astype(jnp.bfloat16)


def solution(mesh):
    in_specs = (
        P(("rep", "fs"), "tp"),
        P("fs", "tp"),
        P("fs", "tp"),
        P("tp", None, None),
        P("tp", None, None),
        P("tp"),
        P(None, "tp"),
        P(("rep", "fs"), "tp"),
        P("tp", "fs"),
        P("fs", "tp"),
        P("fs", "tp"),
        P(None, "tp"),
        P(None, "tp"),
        P("tp", "fs"),
        P(),
        P(),
        P(),
    )
    out_specs = P(("rep", "fs"), "tp")
    ringed = mesh.shape["rep"] == 2 and mesh.shape["tp"] == 2 and mesh.shape["fs"] == 8
    body = functools.partial(shards, ringed)
    return jax.shard_map(body, mesh=mesh, in_specs=in_specs, out_specs=out_specs, check_vma=False)
```

```python
import functools

import jax
import jax.numpy as jnp
from jax import lax
from jax.experimental import pallas as pl
from jax.experimental.pallas import tpu as pltpu
from jax.sharding import PartitionSpec as P

EPS = 1e-06
GATE_POWER = 8.0


def rms_scale(row_block, gain_vec):
    widened = row_block.astype(jnp.float32)
    inverse = lax.rsqrt(jnp.mean(widened * widened, axis=-1, keepdims=True) + EPS)
    return (widened * inverse * gain_vec).astype(jnp.bfloat16)


def causal_mix(values, kernel_taps):
    extent = kernel_taps.shape[0]
    length = values.shape[0]
    padded = jnp.pad(values, ((extent - 1, 0), (0, 0)))
    summed = kernel_taps[0] * padded[0:length]
    for offset in range(1, extent):
        summed = summed + kernel_taps[offset] * padded[offset : offset + length]
    return summed


def chain_step(earlier, following):
    return (earlier[0] * following[0], following[0] * earlier[1] + following[1])


def fold_pair(source, pieces):
    return (
        jnp.dot(source, pieces[0], preferred_element_type=jnp.float32),
        jnp.dot(source, pieces[1], preferred_element_type=jnp.float32),
    )


def project_with(left_rows, weight_piece):
    return jnp.dot(left_rows, weight_piece, preferred_element_type=jnp.float32).astype(jnp.bfloat16)


class PairGather:
    def __init__(self, n, sources, targets, shifts, sems):
        self.n = n
        self.shifts = shifts
        self.sources = sources
        self.targets = targets
        (self.local_sem, self.y_send, self.y_recv, self.z_send, self.z_recv, self.x_send, self.x_recv) = sems
        self.x = lax.axis_index("rep")
        fs = lax.axis_index("fs")
        self.y = lax.rem(fs, 2)
        self.z = fs // 2
        levels = n // 2
        self.middle = self.z * (levels - 1 - self.z) // (levels - 2)
        self.inner = self.middle == 1

    def level(self, k):
        levels = self.n // 2
        across = levels - 1 - self.z
        beyond = lax.rem(self.z + levels // 2, levels)
        if k == 0:
            return self.z
        if k == 1:
            return self.z + 1 - 2 * lax.rem(self.z, 2)
        if k == 2:
            return self.middle * across + (1 - self.middle) * beyond
        return self.middle * beyond + (1 - self.middle) * across

    def side(self, q):
        return lax.rem(self.y + q, 2)

    def member(self, k, q):
        return 2 * self.level(k) + self.side(q)

    def enter(self):
        barrier = pltpu.get_barrier_semaphore()
        devices = [
            {"rep": 1 - self.x},
            {"tp": 1 - lax.axis_index("tp")},
            {"fs": self.member(0, 1)},
            {"fs": self.member(1, 0)},
        ]
        for device in devices:
            pl.semaphore_signal(
                barrier, inc=1, device_id=device, device_id_type=pl.DeviceIdType.MESH
            )

        @pl.when(self.inner)
        def _():
            pl.semaphore_signal(
                barrier,
                inc=1,
                device_id={"fs": self.member(2, 0)},
                device_id_type=pl.DeviceIdType.MESH,
            )

        pl.semaphore_wait(barrier, len(devices) + self.middle)

    def depth(self, w):
        return self.targets[w].shape[0] // self.n

    def source(self, w, half, r):
        ref, depth = self.sources[w], self.depth(w)
        part = depth // 2
        cols = self.targets[w].shape[1]
        if ref.shape[0] == depth:
            lower = half * (ref.shape[1] // 2) + self.shifts[w]
            return ref.at[
                pl.ds(pl.multiple_of(r * part, 16), part),
                pl.ds(pl.multiple_of(lower, 128), cols),
            ]
        lower = half * depth + r * part
        return ref.at[pl.ds(pl.multiple_of(lower, 16), part), pl.ds(self.shifts[w], cols)]

    def piece(self, w, shard, r):
        depth = self.depth(w)
        part = depth // 2
        return self.targets[w].at[pl.ds(pl.multiple_of(shard * depth + r * part, 16), part), :]

    def copy(self, source, target, send_sem, recv_sem, device):
        return pltpu.make_async_remote_copy(
            src_ref=source,
            dst_ref=target,
            send_sem=send_sem,
            recv_sem=recv_sem,
            device_id=device,
            device_id_type=pl.DeviceIdType.MESH,
        )

    def half_of(self, i):
        return self.x if i == 0 else 1 - self.x

    def local(self, w, i):
        r = self.half_of(i)
        return pltpu.make_async_copy(
            self.source(w, self.y, r), self.piece(w, self.member(0, 0), r), self.local_sem.at[w, i]
        )

    def y_copy(self, w, i):
        r = self.half_of(i)
        return self.copy(
            self.source(w, 1 - self.y, r),
            self.piece(w, self.member(0, 0), r),
            self.y_send.at[w, i],
            self.y_recv.at[w, i],
            {"fs": self.member(0, 1)},
        )

    def y_arrival(self, w, i):
        target = self.piece(w, self.member(0, 1), self.half_of(i))
        return self.copy(
            target, target, self.y_send.at[w, i], self.y_recv.at[w, i], {"fs": self.member(0, 1)}
        )

    def hop(self, w, q, k, level):
        shard = self.member(k, q)
        target = self.piece(w, shard, self.x)
        source = self.source(w, self.y, self.x) if k == 0 and q == 0 and w > 0 else target
        step = level - self.level(k)
        lane = step + self.n // 2 - 1
        return self.copy(
            source,
            target,
            self.z_send.at[w, q, lane],
            self.z_recv.at[w, q, lane],
            {"fs": 2 * level + self.y},
        )

    def z_arrival(self, w, q, k):
        target = self.piece(w, self.member(k, q), self.x)
        lane = self.z - self.level(k) + self.n // 2 - 1
        return self.copy(
            target,
            target,
            self.z_send.at[w, q, lane],
            self.z_recv.at[w, q, lane],
            {"fs": self.member(1, 0)},
        )

    def onward(self, w, q, k):
        level = self.level(2) if k == 1 else self.level(1)
        return self.hop(w, q, k, level)

    def x_copy(self, w, q, k):
        target = self.piece(w, self.member(k, q), self.x)
        return self.copy(
            target, target, self.x_send.at[w, q, k], self.x_recv.at[w, q, k], {"rep": 1 - self.x}
        )

    def x_arrival(self, w, q, k):
        target = self.piece(w, self.member(k, q), 1 - self.x)
        return self.copy(
            target, target, self.x_send.at[w, q, k], self.x_recv.at[w, q, k], {"rep": 1 - self.x}
        )

    def end_start(self, w, q):
        @pl.when(jnp.logical_not(self.inner))
        def _():
            self.hop(w, q, 0, self.level(1)).start()

    def inner_start(self, w, q):
        @pl.when(self.inner)
        def _():
            self.hop(w, q, 0, self.level(1)).start()
            self.hop(w, q, 0, self.level(2)).start()

    def z_start(self, w, q):
        self.hop(w, q, 0, self.level(1)).start()

        @pl.when(self.inner)
        def _():
            self.hop(w, q, 0, self.level(2)).start()

    def edge_start(self, w, q):
        self.hop(w, q, 0, self.level(1)).start()

    def core_start(self, w, q):
        @pl.when(self.inner)
        def _():
            self.hop(w, q, 0, self.level(2)).start()

    def crossed(self, w):
        self.y_arrival(w, 0).wait_recv()

    def cross(self, w):
        self.crossed(w)
        self.z_start(w, 1)

    def serve(self, w, q, k):
        self.z_arrival(w, q, k).wait_recv()

        @pl.when(self.inner)
        def _():
            self.onward(w, q, k).start()

        self.x_copy(w, q, k).start()

    def split_serve(self, at_end, at_inner):
        @pl.when(self.inner)
        def _():
            w, k, q = at_inner
            self.z_arrival(w, q, k).wait_recv()
            self.onward(w, q, k).start()
            self.x_copy(w, q, k).start()

        @pl.when(jnp.logical_not(self.inner))
        def _():
            w, k, q = at_end
            self.z_arrival(w, q, k).wait_recv()
            self.x_copy(w, q, k).start()

    def own_ready(self, w):
        if w > 0:
            self.local(w, 0).wait()
        self.local(w, 1).wait()
        self.y_arrival(w, 1).wait_recv()

    def ready(self, w):
        self.own_ready(w)
        for q in (0, 1):
            for k in (1, 2, 3):
                self.x_arrival(w, q, k).wait_recv()

    def drain(self, w):
        for i in (0, 1):
            self.y_copy(w, i).wait_send()
        for q in (0, 1):
            self.hop(w, q, 0, self.level(1)).wait_send()
            for k in (1, 2, 3):
                self.x_copy(w, q, k).wait_send()

            @pl.when(self.inner)
            def _():
                self.hop(w, q, 0, self.level(2)).wait_send()
                for k in (1, 2, 3):
                    self.onward(w, q, k).wait_send()


def gelu_of(x):
    return 0.5 * x * (1.0 + jnp.tanh(0.7978845608028654 * (x + 0.044715 * (x * x * x))))


def one_less_exp(z):
    series = 1.0 + z * (1.0 / 6.0)
    for order in (5.0, 4.0, 3.0, 2.0):
        series = 1.0 + z * (1.0 / order) * series
    return jnp.where(z > -0.35, -z * series, 1.0 - jnp.exp(z))


def tap_rows(values, taps_ref, cols):
    extent = taps_ref.shape[0]
    summed = taps_ref[extent - 1 : extent, cols] * values
    row = lax.broadcasted_iota(jnp.int32, values.shape, 0)
    for back in range(1, extent):
        moved = jnp.where(row >= back, pltpu.roll(values, back, 0), 0.0)
        summed = summed + taps_ref[extent - 1 - back : extent - back, cols] * moved
    return summed


def dot32(a, b):
    return jnp.dot(a, b, preferred_element_type=jnp.float32)


def layer_kernel(n, *refs):
    sources = [refs[i] for i in (0, 1, 2, 3, 3, 4, 4, 5, 5)]
    (stream, reset_map, admit_map, decay_rate, taps, spike) = refs[6:12]
    (gate_taps, value_taps, rec_gain, ffn_gain, last_gain, out) = refs[12:18]
    targets = refs[18:27]
    (whole, spike_in, normed, gate_src, decay, inflow, mixed) = refs[27:34]
    (away, landed, kept, share, share_in, middle, middle_in, gate_up, hidden) = refs[34:43]
    (terms, landed_down, down, down_own, down_in, final, sums, sums_in) = refs[43:51]
    gather_sems = refs[51:58]
    (keep_sem, pair_send, pair_recv, near_send, near_recv, far_send, far_recv) = refs[58:]
    tokens, width = stream.shape
    me = lax.axis_index("tp")
    wide_cut, down_cut = targets[3].shape[1], targets[7].shape[1]
    shifts = [0, 0, 0, 0, wide_cut, 0, wide_cut, 0, down_cut]
    gather = PairGather(n, sources, targets, shifts, gather_sems)
    last = len(targets) - 1
    side = gather.y
    bf16, f32 = jnp.bfloat16, jnp.float32
    tile = 256
    strip = 48
    channels = width // 2
    units = hidden.shape[1]
    chunks = 4
    chunk = 2 * tokens // chunks

    def near(i, source, target):
        return gather.copy(source, target, near_send.at[i], near_recv.at[i], {"tp": 1 - me})

    def far(i, source, target):
        return gather.copy(
            source, target, far_send.at[i], far_recv.at[i], {"fs": gather.member(0, 1)}
        )

    def pair(i, source, target):
        return gather.copy(source, target, pair_send.at[i], pair_recv.at[i], {"tp": 1 - me})

    def half(which):
        return pl.ds(pl.multiple_of(which * width, 128), width)

    def strips(lower, upper, body):
        def step(i, carry):
            body(pl.ds(pl.multiple_of(lower + i * strip, 16), strip))
            return carry

        lax.fori_loop(0, (upper - lower) // strip, step, 0)

    def norm_rows(lower, upper, mine, theirs, gain):
        def body(rows):
            a = mine(rows).astype(f32)
            b = theirs(rows).astype(f32)
            total = jnp.sum(a * a, axis=1, keepdims=True) + jnp.sum(b * b, axis=1, keepdims=True)
            inverse = lax.rsqrt(total * (1.0 / (2 * width)) + EPS)
            normed[rows, half(me)] = (a * inverse * gain[:, half(me)]).astype(bf16)
            normed[rows, half(1 - me)] = (b * inverse * gain[:, half(1 - me)]).astype(bf16)

        strips(lower, upper, body)

    first_rows, second_rows = pl.ds(0, tokens), pl.ds(tokens, tokens)
    mine_in = lambda rows: whole[rows, half(me)]
    theirs_in = lambda rows: whole[rows, half(1 - me)]

    arrivals = [(k, q) for k in (1, 2, 3) for q in (0, 1)]
    opening = [(0, 1, 0), (1, 1, 0), (0, 1, 1), (0, 2, 0), (1, 1, 1), (0, 2, 1), (0, 3, 0), (0, 3, 1)]
    inner_opening = [opening[i] for i in (0, 3, 2, 5, 1, 4, 6, 7)]
    steady = []
    for w in range(1, last + 1):
        steady += [(w, 2, 0), (w, 2, 1)]
        for q in (0, 1):
            steady.append((w, 3, q))
            if w < last:
                steady.append((w + 1, 1, q))
    plan, inner_plan = opening + steady, inner_opening + steady
    served = [0]

    def pump(upto):
        while served[0] < upto:
            w, k, q = plan[served[0]]
            if plan[served[0]] == inner_plan[served[0]]:
                gather.serve(w, q, k)
            else:
                gather.split_serve(plan[served[0]], inner_plan[served[0]])
            served[0] += 1
            if 0 < w < last:
                if (k, q) == (1, 1):
                    gather.end_start(w + 1, 0)
                if (k, q) == (2, 1):
                    gather.crossed(w + 1)
                    gather.end_start(w + 1, 1)
                if k == 3:
                    gather.inner_start(w + 1, q)
            if served[0] == 4:
                gather.y_copy(3, 0).start()
                sent_spike.start()
                gather.y_copy(2, 1).start()
                gather.y_copy(4, 0).start()
            if served[0] == 9:
                for later in (5, 6, 7, 8):
                    gather.y_copy(later, 0).start()
                for later in (3, 4):
                    gather.y_copy(later, 1).start()

    sent_spike = far(1, spike, spike_in)
    gather.local(0, 0).start()
    gather.enter()
    gather.local(0, 0).wait()
    gather.z_start(0, 0)
    gather.y_copy(0, 0).start()
    gather.y_copy(1, 0).start()
    gather.y_copy(2, 0).start()
    own_half = near(0, stream, whole.at[first_rows, half(me)])
    own_half.start()
    sent_half = far(0, stream, whole.at[second_rows, half(me)])
    sent_half.start()
    gather.y_copy(0, 1).start()
    gather.y_copy(1, 1).start()
    keep = pltpu.make_async_copy(stream, whole.at[first_rows, half(me)], keep_sem.at[0])
    keep.start()
    gather.edge_start(1, 0)
    gather.local(0, 1).start()
    for w in range(1, last + 1):
        for i in (0, 1):
            gather.local(w, i).start()
    gather.cross(0)
    pump(2)
    gather.core_start(1, 0)
    gather.cross(1)
    pump(8)
    keep.wait()
    own_half.wait()
    norm_rows(0, tokens, mine_in, theirs_in, rec_gain)
    pump(10)
    sent_half.wait()
    passed = whole.at[second_rows, half(me)]
    pass_on = near(1, passed, passed)
    pass_on.start()
    pump(11)
    pass_on.wait()
    norm_rows(tokens, 2 * tokens, mine_in, theirs_in, rec_gain)
    pump(16)
    gather.ready(0)
    gather.ready(1)
    sent_spike.wait()

    events_of = [spike[...].T, spike_in[...].T]
    row_sets = [pl.ds(s * tokens, tokens) for s in (0, 1)]
    base = side * channels

    def decay_base(cols):
        rate = -decay_rate[:, cols]
        return GATE_POWER * (jnp.maximum(rate, 0.0) + jnp.log1p(jnp.exp(-jnp.abs(rate))))

    def wide(start, size):
        return pl.ds(pl.multiple_of(start, 128), size)

    for c in range(channels // tile):
        cols = slice(c * tile, (c + 1) * tile)
        for s in (0, 1):
            rows = row_sets[s]
            rec = dot32(normed[rows, :], targets[0][:, cols]).astype(bf16).astype(f32)
            conv = tap_rows(rec, taps, wide(base + c * tile, tile)).astype(bf16)
            gate_src[rows, cols] = dot32(normed[rows, :], targets[1][:, cols]).astype(bf16)
            spikes = events_of[s]
            for part in range(tile // 128):
                h = c * (tile // 128) + part
                heads = channels // 128
                lanes = slice(h * 128, (h + 1) * 128)
                block = conv[:, part * 128 : (part + 1) * 128]
                reset = jax.nn.sigmoid(dot32(block, reset_map[side * heads + h]))
                admit = jax.nn.sigmoid(dot32(block, admit_map[side * heads + h]))
                events = jnp.where(
                    side == 0, spikes[:, h : h + 1], spikes[:, heads + h : heads + h + 1]
                )
                log_decay = events - reset * decay_base(wide(base + h * 128, 128))
                decay[rows, lanes] = jnp.exp(log_decay)
                inflow[rows, lanes] = (
                    jnp.sqrt(one_less_exp(2.0 * log_decay)) * admit * block.astype(f32)
                )
            pump(17 + c)

    row = lax.broadcasted_iota(jnp.int32, (8, channels), 0)

    def scan_step(i, carry):
        passed_on = []
        for s in (0, 1):
            rows = pl.ds(pl.multiple_of(s * tokens + i * 16, 16), 16)
            a16, b16 = decay[rows, :], inflow[rows, :]
            state = carry[s]
            found = []
            for part in range(2):
                a, b = a16[part * 8 : part * 8 + 8], b16[part * 8 : part * 8 + 8]
                for back in (1, 2, 4):
                    a_before = jnp.where(row >= back, pltpu.roll(a, back, 0), 1.0)
                    b_before = jnp.where(row >= back, pltpu.roll(b, back, 0), 0.0)
                    b = a * b_before + b
                    a = a * a_before
                states = a * state + b
                state = states[7:8, :]
                found.append(states)
            states = jnp.concatenate(found, axis=0)
            mixed[rows, :] = (states * gelu_of(gate_src[rows, :].astype(f32))).astype(bf16)
            passed_on.append(state)
        return tuple(passed_on)

    still = jnp.zeros((1, channels), f32)
    halfway = tokens // 32
    carry = lax.fori_loop(0, halfway, scan_step, (still, still))
    pump(19)
    lax.fori_loop(halfway, tokens // 16, scan_step, carry)
    pump(20)
    gather.ready(2)

    per_half = n // 2
    depth = channels

    def block_of(w, slot, depth):
        return targets[w][pl.ds(pl.multiple_of(slot * depth, 16), depth), :]

    def away_step(j, carry):
        cols = wide(j * tile, tile)
        away[:, cols] = dot32(mixed[...], block_of(2, (1 - me) * per_half + j, depth)).astype(bf16)
        near(2 + j, away.at[:, cols], landed.at[:, cols]).start()
        return carry

    def keep_step(j, carry):
        cols = wide(j * tile, tile)
        kept[:, cols] = dot32(mixed[...], block_of(2, me * per_half + j, depth)).astype(bf16)
        return carry

    lax.fori_loop(0, per_half, away_step, 0)
    pump(21)
    lax.fori_loop(0, per_half, keep_step, 0)
    pump(22)
    for j in range(per_half):
        cols = slice(j * tile, (j + 1) * tile)
        near(2 + j, away.at[:, cols], landed.at[:, cols]).wait()

    def share_rows(rows):
        share[rows, :] = (kept[rows, :].astype(f32) + landed[rows, :].astype(f32)).astype(bf16)

    def share_copy(i):
        rows = pl.ds((i + chunks // 2) % chunks * chunk, chunk)
        return far(2 + i, share.at[rows, :], share_in.at[pl.ds(i * chunk, chunk), :])

    def middle_copy(i):
        rows = pl.ds(i * chunk, chunk)
        return pair(i, middle.at[rows, :], middle_in.at[rows, :])

    for i in range(chunks):
        lower = (i + chunks // 2) % chunks * chunk
        strips(lower, lower + chunk, share_rows)
        share_copy(i).start()
    for later in (5, 6, 7, 8):
        gather.y_copy(later, 1).start()

    def add_branch(rows):
        branch = (share[rows, :].astype(f32) + share_in[rows, :].astype(f32)).astype(bf16)
        middle[rows, :] = (whole[rows, half(me)].astype(f32) + branch.astype(f32)).astype(bf16)

    for i in range(chunks):
        pump((26, 29, 32, 35)[i])
        share_copy(i).wait()
        strips(i * chunk, (i + 1) * chunk, add_branch)
        middle_copy(i).start()
        pump((27, 30, 33, 36)[i])
        middle_copy(i).wait()
        norm_rows(
            i * chunk,
            (i + 1) * chunk,
            lambda rows: middle[rows, :],
            lambda rows: middle_in[rows, :],
            ffn_gain,
        )
    gather.ready(3)
    gather.ready(4)

    unit_base = side * units
    tiles = units // tile
    per_cut = wide_cut // tile

    def gate_step(j):
        inside = slice(j % per_cut * tile, (j % per_cut + 1) * tile)
        block = targets[3 + j // per_cut][:, inside]
        gate_up[:, j * tile : (j + 1) * tile] = dot32(normed[...], block).astype(bf16)

    def up_step(j):
        cols = slice(j * tile, (j + 1) * tile)
        inside = slice(j % per_cut * tile, (j % per_cut + 1) * tile)
        picked = wide(unit_base + j * tile, tile)
        for s in (0, 1):
            rows = row_sets[s]
            block = targets[5 + j // per_cut][:, inside]
            value = dot32(normed[rows, :], block).astype(bf16).astype(f32)
            value = tap_rows(value, value_taps, picked)
            gate = gelu_of(tap_rows(gate_up[rows, cols].astype(f32), gate_taps, picked))
            hidden[rows, cols] = (gate * value).astype(bf16)

    for j in range(tiles):
        gate_step(j)
        pump((37, 38, 38, 39)[j])
    gather.ready(5)
    for j in range(tiles):
        if j == per_cut:
            pump(45)
            gather.ready(6)
        up_step(j)
        pump((40, 41, 46, 47)[j])

    low = gather.z // 2
    order = [(cut, k, q) for cut in (0, 1) for k, q in [(0, 0), (0, 1)] + arrivals]

    def owned(k):
        return (me == low) if k in (0, 1) else (me == 1 - low)

    def slot_of(i):
        return gather.member(order[i][1], order[i][2])

    def cols_of(i):
        return wide(slot_of(i) * tile + order[i][0] * down_cut, down_cut)

    def place_of(i):
        return wide(lax.rem(slot_of(i), per_half) * tile + order[i][0] * down_cut, down_cut)

    def down_copy(i, s):
        cols = cols_of(i)
        rows = row_sets[s]
        return near(
            2 + per_half + 2 * i + s, terms.at[rows, cols], landed_down.at[rows, place_of(i)]
        )

    def down_far(i):
        place = place_of(i)
        at = 2 + chunks + 2 * lax.rem(slot_of(i), per_half) + order[i][0]
        return gather.copy(
            down.at[:, place],
            down_in.at[:, place],
            far_send.at[at],
            far_recv.at[at],
            {"fs": gather.member(0, 1)},
        )

    block_rows = 128

    def blocks(body):
        def step(r, carry):
            body(pl.multiple_of(r * block_rows, 16))
            return carry

        lax.fori_loop(0, tokens // block_rows, step, 0)

    def fold(i, s):
        @pl.when(owned(order[i][1]))
        def _():
            cols, place = cols_of(i), place_of(i)

            def folded(lower):
                rows = pl.ds(lower, block_rows)
                return (terms[rows, cols].astype(f32) + landed_down[rows, place].astype(f32)).astype(
                    bf16
                )

            def far_rows(lower):
                down[pl.ds(lower, block_rows), place] = folded(tokens + lower)

            def own_rows(lower):
                down_own[pl.ds(lower, block_rows), place] = folded(lower)

            if s == 1:
                down_copy(i, 1).wait_recv()
                blocks(far_rows)
                down_far(i).start()
            else:
                down_copy(i, 0).wait_recv()
                blocks(own_rows)

    def finish(i):
        @pl.when(owned(order[i][1]))
        def _():
            place = place_of(i)
            down_far(i).wait()

            def body(lower):
                rows = pl.ds(lower, block_rows)
                branch = down_own[rows, place].astype(f32) + down_in[rows, place].astype(f32)
                total = middle[rows, place].astype(f32) + branch.astype(bf16).astype(f32)
                final[rows, place] = total * last_gain[:, wide(me * width + place.start, down_cut)]
                square = jnp.sum(total * total, axis=1, keepdims=True)
                before = 0.0 if i in (0, per_half) else sums[rows, :]
                sums[rows, :] = before + jnp.broadcast_to(square, (block_rows, 128))

            blocks(body)

    for i in range(len(order)):
        cut, k, q = order[i]
        if i == 0:
            gather.own_ready(7)
            gather.own_ready(8)
        pump((47, 47, 48, 48, 49, 49, 50, 51, 51, 52, 52, 53, 53, 54, 54, 54)[i])
        if k > 0:
            gather.x_arrival(7 + cut, q, k).wait_recv()
        cols = cols_of(i)
        for s in (1, 0):
            rows = row_sets[s]
            block = block_of(7 + cut, slot_of(i), units)
            terms[rows, cols] = dot32(hidden[rows, :], block).astype(bf16)

            @pl.when(jnp.logical_not(owned(k)))
            def _():
                down_copy(i, s).start()

            if i > 0:
                fold(i - 1, s)
    for s in (1, 0):
        fold(len(order) - 1, s)
    for i in range(len(order)):
        finish(i)
    for i in range(len(order)):

        @pl.when(jnp.logical_not(owned(order[i][1])))
        def _():
            for s in (0, 1):
                down_copy(i, s).wait_send()

    summed = pair(chunks, sums, sums_in)
    summed.start()
    summed.wait()

    def scale(lower):
        rows = pl.ds(lower, block_rows)
        square = sums[rows, :] + sums_in[rows, :]
        inverse = lax.rsqrt(square * (1.0 / (2 * width)) + EPS)[:, 0:1]
        out[rows, :] = (final[rows, :] * inverse).astype(bf16)

    blocks(scale)
    for w in range(last + 1):
        gather.drain(w)


def fused_layer(n, weights, others):
    tokens, width = others[0].shape
    units = weights[3].shape[1] // 2
    channels = width // 2
    bf16, f32 = jnp.bfloat16, jnp.float32
    vmem = pltpu.VMEM
    dma = pltpu.SemaphoreType.DMA
    halves = []
    for w in weights:
        if w.shape[0] == 2 * width // n:
            halves.append((n * w.shape[0], w.shape[1] // 2))
        else:
            halves.append((n * w.shape[0] // 2, w.shape[1]))
    split = [(rows, cols // 2) for rows, cols in halves[3:5] for _ in (0, 1)]
    halves = halves[:3] + split + [(halves[5][0], halves[5][1] // 2)] * 2
    parts = len(halves)
    both = 2 * tokens
    return pl.pallas_call(
        functools.partial(layer_kernel, n),
        out_shape=jax.ShapeDtypeStruct((tokens, width), bf16),
        in_specs=[pl.BlockSpec(memory_space=pl.ANY)] * 6
        + [pl.BlockSpec(memory_space=vmem)] * len(others),
        out_specs=pl.BlockSpec(memory_space=vmem),
        scratch_shapes=[vmem(shape, bf16) for shape in halves]
        + [
            vmem((both, 2 * width), bf16),
            vmem(others[5].shape, f32),
            vmem((both, 2 * width), bf16),
            vmem((both, channels), bf16),
            vmem((both, channels), f32),
            vmem((both, channels), f32),
            vmem((both, channels), bf16),
            vmem((both, width), bf16),
            vmem((both, width), bf16),
            vmem((both, width), bf16),
            vmem((both, width), bf16),
            vmem((both, width), bf16),
            vmem((both, width), bf16),
            vmem((both, width), bf16),
            vmem((both, units), bf16),
            vmem((both, units), bf16),
            vmem((both, 2 * width), bf16),
            vmem((both, width), bf16),
            vmem((tokens, width), bf16),
            vmem((tokens, width), bf16),
            vmem((tokens, width), bf16),
            vmem((tokens, width), f32),
            vmem((tokens, 128), f32),
            vmem((tokens, 128), f32),
            dma((parts, 2)),
            dma((parts, 2)),
            dma((parts, 2)),
            dma((parts, 2, n - 1)),
            dma((parts, 2, n - 1)),
            dma((parts, 2, 4)),
            dma((parts, 2, 4)),
            dma((1,)),
            dma((5,)),
            dma((5,)),
            dma((2 + n // 2 + 4 * n,)),
            dma((2 + n // 2 + 4 * n,)),
            dma((6 + n,)),
            dma((6 + n,)),
        ],
        compiler_params=pltpu.CompilerParams(
            collective_id=0, has_side_effects=True, vmem_limit_bytes=66_000_000
        ),
    )(*weights, *others)


def shards(
    ringed,
    stream,
    recurrence_input_weight,
    output_gate_weight,
    recurrence_gate_matrix,
    input_gate_matrix,
    channel_decay_rate,
    recurrence_taps,
    spike_log_decay,
    recurrence_output_weight,
    feedforward_gate_upward,
    feedforward_value_upward,
    feedforward_gate_taps,
    feedforward_value_taps,
    feedforward_down_weight,
    recurrence_norm_gain,
    feedforward_norm_gain,
    closing_norm_gain,
):
    tok_rows = stream.shape[0]
    fs_size = lax.axis_size("fs")
    if ringed:
        return fused_layer(
            fs_size,
            (
                recurrence_input_weight,
                output_gate_weight,
                recurrence_output_weight,
                feedforward_gate_upward,
                feedforward_value_upward,
                feedforward_down_weight,
            ),
            (
                stream,
                recurrence_gate_matrix,
                input_gate_matrix,
                channel_decay_rate[None, :],
                recurrence_taps,
                spike_log_decay.T,
                feedforward_gate_taps,
                feedforward_value_taps,
                recurrence_norm_gain[None, :],
                feedforward_norm_gain[None, :],
                closing_norm_gain[None, :],
            ),
        )
    weights = [
        lax.all_gather(recurrence_input_weight, "fs", axis=0, tiled=True),
        lax.all_gather(output_gate_weight, "fs", axis=0, tiled=True),
        lax.all_gather(recurrence_output_weight, "fs", axis=1, tiled=True),
        lax.all_gather(feedforward_gate_upward, "fs", axis=0, tiled=True),
        lax.all_gather(feedforward_value_upward, "fs", axis=0, tiled=True),
        lax.all_gather(feedforward_down_weight, "fs", axis=1, tiled=True),
    ]
    head_count = recurrence_gate_matrix.shape[0]
    block_size = recurrence_gate_matrix.shape[1]
    whole_rows = lax.all_gather(stream, "tp", axis=1, tiled=True)
    normed = rms_scale(whole_rows, recurrence_norm_gain)
    rec_sum, gate_sum = fold_pair(
        normed,
        (
            weights[0],
            weights[1],
        ),
    )
    rec_in = rec_sum.astype(jnp.bfloat16)
    gate_src = gate_sum.astype(jnp.bfloat16)
    conv_out = causal_mix(rec_in.astype(jnp.float32), recurrence_taps).astype(jnp.bfloat16)
    blocks = conv_out.reshape(tok_rows, head_count, block_size)
    gate_restart = jax.nn.sigmoid(
        jnp.einsum(
            "thi,hij->thj", blocks, recurrence_gate_matrix, preferred_element_type=jnp.float32
        )
    )
    admit_gate = jax.nn.sigmoid(
        jnp.einsum("thi,hij->thj", blocks, input_gate_matrix, preferred_element_type=jnp.float32)
    )
    decay_base = (GATE_POWER * jax.nn.softplus(-channel_decay_rate)).reshape(head_count, block_size)
    decay_logarithm = -gate_restart * decay_base + spike_log_decay[:, :, None]
    decay_rate = jnp.exp(decay_logarithm)
    inflow = jnp.sqrt(-jnp.expm1(2.0 * decay_logarithm)) * admit_gate * blocks.astype(jnp.float32)
    states = lax.associative_scan(chain_step, (decay_rate, inflow), axis=0)[1]
    mixed_out = (
        states.reshape(tok_rows, head_count * block_size)
        * jax.nn.gelu(gate_src.astype(jnp.float32))
    ).astype(jnp.bfloat16)
    mix_terms = project_with(
        mixed_out, weights[2]
    )
    branch = lax.psum_scatter(
        lax.optimization_barrier(mix_terms).astype(jnp.float32).astype(jnp.bfloat16),
        "tp",
        scatter_dimension=1,
        tiled=True,
    )
    middle = (stream.astype(jnp.float32) + branch.astype(jnp.float32)).astype(jnp.bfloat16)
    whole_middle = lax.all_gather(middle, "tp", axis=1, tiled=True)
    normed_ffn = rms_scale(whole_middle, feedforward_norm_gain)
    gate_sum_ffn, value_sum_ffn = fold_pair(
        normed_ffn,
        (
            weights[3],
            weights[4],
        ),
    )
    gate_up = gate_sum_ffn.astype(jnp.bfloat16)
    value_up = value_sum_ffn.astype(jnp.bfloat16)
    gate_conv = causal_mix(gate_up.astype(jnp.float32), feedforward_gate_taps)
    value_conv = causal_mix(value_up.astype(jnp.float32), feedforward_value_taps)
    hidden = (jax.nn.gelu(gate_conv) * value_conv).astype(jnp.bfloat16)
    down_terms = project_with(
        hidden, weights[5]
    )
    branch_ffn = lax.psum_scatter(
        lax.optimization_barrier(down_terms).astype(jnp.float32).astype(jnp.bfloat16),
        "tp",
        scatter_dimension=1,
        tiled=True,
    )
    final_rows = middle.astype(jnp.float32) + branch_ffn.astype(jnp.float32)
    col_count = final_rows.shape[1]
    square_sum = lax.psum(jnp.sum(final_rows * final_rows, axis=1), "tp")
    inverse = lax.rsqrt(square_sum / (col_count * lax.axis_size("tp")) + EPS)
    gain_part = lax.dynamic_slice_in_dim(
        closing_norm_gain, lax.axis_index("tp") * col_count, col_count
    )
    return (final_rows * inverse[:, None] * gain_part[None, :]).astype(jnp.bfloat16)


def solution(mesh):
    in_specs = (
        P(("rep", "fs"), "tp"),
        P("fs", "tp"),
        P("fs", "tp"),
        P("tp", None, None),
        P("tp", None, None),
        P("tp"),
        P(None, "tp"),
        P(("rep", "fs"), "tp"),
        P("tp", "fs"),
        P("fs", "tp"),
        P("fs", "tp"),
        P(None, "tp"),
        P(None, "tp"),
        P("tp", "fs"),
        P(),
        P(),
        P(),
    )
    out_specs = P(("rep", "fs"), "tp")
    ringed = mesh.shape["rep"] == 2 and mesh.shape["tp"] == 2 and mesh.shape["fs"] == 8
    body = functools.partial(shards, ringed)
    return jax.shard_map(body, mesh=mesh, in_specs=in_specs, out_specs=out_specs, check_vma=False)
```
